128 devices in a mesh: dp: 4 (over x), kv: 16 (over z, y), tp: 2 (over core).
Axes of the slice: x: 4, y: 4, z: 4, core: 2. Of those that a mesh axis runs over, the one named last changes fastest.
Arguments:
- pieces: bfloat16 [4096, 8, 2048], P(('kv', 'tp'), 'dp'), parts along dimension 1, may hold values from -6 to 6
- new_tokens: bfloat16 [256, 2048], P(('dp', 'kv', 'tp')), parts along dimension 0, may hold values from -6 to 6
- w_query: bfloat16 [2048, 1024], P(None, 'tp'), may hold values from -0.125 to 0.125
- w_key: bfloat16 [2048, 1024], P(None, 'tp'), may hold values from -0.125 to 0.125
- w_value: bfloat16 [2048, 2048], P(None, 'tp'), may hold values from -0.125 to 0.125
- w_decay: bfloat16 [2048, 1024], P(None, 'tp'), may hold values from -0.125 to 0.125
- decay_bias: float32 [1024], replicated, may hold values from 0 to 9
- norm_gain: float32 [2048], replicated, may hold values from 0.1 to 1.9
- head_gain: float32 [2048], replicated, may hold values from 0.1 to 1.9
- w_out: bfloat16 [2048, 2048], replicated, may hold values from -0.125 to 0.125
- prompt_state: float32 [8, 8, 128, 256], P('dp', 'tp', 'kv'), parts along dimension 0, may hold values from -8 to 8
- decode_state: float32 [256, 8, 128, 256], P(('dp', 'kv'), 'tp'), parts along dimension 0, may hold values from -8 to 8
Outputs:
- mixed_piece: bfloat16 [4096, 8, 2048], P(('kv', 'tp'), 'dp'), parts along dimension 1
- mixed_decode: bfloat16 [256, 2048], P(('dp', 'kv', 'tp')), parts along dimension 0
- prompt_state_out: float32 [8, 8, 128, 256], P('dp', 'tp', 'kv'), parts along dimension 0
- decode_state_out: float32 [256, 8, 128, 256], P(('dp', 'kv'), 'tp'), parts along dimension 0
The draws below stay inside these ranges and needn't reach their ends.
There are 4 independent parts, one for each index of `dp`. The reference program is written for one: setup_inputs(seed, part) draws one part's arguments, and reference() takes and returns one part's arrays. A program takes and returns all parts, laid end to end along the dimension named above; an argument that names none is the same for every part. Nothing has to cross between parts.
All inputs are finite; a program needn't handle non-finite values.
Results may differ from the reference program's by a relative error of at most 0.014.
Values may be sent and summed in bfloat16 or wider, within the bound.
A program may use at most 128 MiB of HBM per device.

```python
import jax
import jax.numpy as jnp
from jax import lax

D = 2048
HEADS = 8
DK = 128
DV = 256
BLOCK = 64
PROMPTS = 2
PIECE = 4096
DEC = 64


def block_scale(rng, extent, cuts, smallest, high):
    def one(axis_at, blocks):
        draws = jax.random.uniform(jax.random.fold_in(jax.random.fold_in(rng, 6), axis_at), (blocks,), jnp.float32, smallest / len(cuts), high / len(cuts))
        return jnp.repeat(jnp.exp(draws), extent[axis_at] // blocks).reshape((-1,) + (1,) * (len(extent) - axis_at - 1))

    level = one(*cuts[0])
    for cut in cuts[1:]:
        level = level * one(*cut)
    return level


def centred(rng, dims, spread, bound, cuts=(), held_as=jnp.bfloat16):
    values = spread * jax.random.normal(rng, dims, jnp.float32)
    if cuts:
        values = values * block_scale(rng, dims, cuts, -0.22, 0.18)
    return jnp.clip(values, -bound, bound).astype(held_as)


def setup_inputs(seed: int = 0, part: int = 0) -> dict:
    key_of = jax.random.split(jax.random.key(seed), 13)
    own_keys = jax.random.split(jax.random.fold_in(key_of[12], part), 13)
    return {
        "pieces": centred(own_keys[0], (PIECE, PROMPTS, D), 1.0, 6.0, ((0, 32),)),
        "new_tokens": centred(own_keys[1], (DEC, D), 1.0, 6.0, ((0, 32),)),
        "w_query": centred(key_of[2], (D, HEADS * DK), D ** -0.5, 0.125, ((1, 2),)),
        "w_key": centred(key_of[3], (D, HEADS * DK), D ** -0.5, 0.125, ((1, 2),)),
        "w_value": centred(key_of[4], (D, HEADS * DV), D ** -0.5, 0.125, ((1, 2),)),
        "w_decay": centred(key_of[5], (D, HEADS * DK), D ** -0.5, 0.125, ((1, 2),)),
        "decay_bias": jnp.clip(jax.random.uniform(key_of[6], (HEADS * DK,), jnp.float32, 0.0, 9.0), 0.0, 9.0),
        "norm_gain": jnp.clip(1.0 + 0.18 * jax.random.normal(key_of[7], (D,), jnp.float32), 0.1, 1.9),
        "head_gain": jnp.clip(1.0 + 0.18 * jax.random.normal(key_of[8], (HEADS * DV,), jnp.float32), 0.1, 1.9),
        "w_out": centred(key_of[9], (HEADS * DV, D), (HEADS * DV) ** -0.5, 0.125),
        "prompt_state": centred(own_keys[10], (PROMPTS, HEADS, DK, DV), 2.0, 8.0, ((1, 2), (2, 16)), jnp.float32),
        "decode_state": centred(own_keys[11], (DEC, HEADS, DK, DV), 2.0, 8.0, ((0, 16), (1, 2)), jnp.float32),
    }


highest = lax.Precision.HIGHEST
norm_eps = 0.1
decay_tau = 16.0
part_limit = 16

def rms_rows(row_block, gain):
    wide = row_block.astype(jnp.float32)
    factor = lax.rsqrt(lax.optimization_barrier(jnp.mean(wide * wide, axis=-1, keepdims=True)) + norm_eps)
    return (wide * factor * gain).astype(jnp.bfloat16)

def head_norm(outputs, gain):
    factor = lax.rsqrt(lax.optimization_barrier(jnp.mean(outputs * outputs, axis=-1, keepdims=True)) + norm_eps)
    flat = (outputs * factor).reshape(outputs.shape[:-2] + (-1,))
    return (flat * gain).astype(jnp.bfloat16)

def project_roles(row_block, w_query, w_key, w_value, w_decay, decay_bias):
    lead = row_block.shape[:-1]
    queries = (jnp.dot(row_block, w_query, preferred_element_type=jnp.float32) * DK ** (-0.5)).astype(jnp.bfloat16)
    keys_new = jnp.dot(row_block, w_key, preferred_element_type=jnp.float32).astype(jnp.bfloat16)
    values_new = jnp.dot(row_block, w_value, preferred_element_type=jnp.float32).astype(jnp.bfloat16)
    decays = jax.nn.log_sigmoid(jnp.dot(row_block, w_decay, preferred_element_type=jnp.float32) + decay_bias) / decay_tau
    return (queries.reshape(lead + (HEADS, DK)), keys_new.reshape(lead + (HEADS, DK)), values_new.reshape(lead + (HEADS, DV)), decays.reshape(lead + (HEADS, DK)))

def block_terms(q_blk, k_blk, v_blk, g_blk):
    block_len = q_blk.shape[0]
    part_len = min(part_limit, block_len)
    part_count = block_len // part_len
    within = jnp.cumsum(g_blk, axis=0)
    part_ends = within[part_len - 1::part_len]
    anchor = jnp.concatenate([jnp.zeros_like(part_ends[:1]), part_ends[:-1]], axis=0)
    q_wide = q_blk.astype(jnp.float32)
    k_wide = k_blk.astype(jnp.float32)
    q_parts = q_wide.reshape((part_count, part_len) + q_blk.shape[1:])
    w_parts = within.reshape((part_count, part_len) + within.shape[1:])
    near_query = (q_parts * jnp.exp(w_parts - anchor[:, None])).astype(jnp.bfloat16)
    near_key = (k_wide[None] * jnp.exp(anchor[:, None] - within[None])).astype(jnp.bfloat16)
    scores = jnp.einsum('itbhk,isbhk->ibhts', near_query, near_key, preferred_element_type=jnp.float32)
    row_pos = jnp.arange(part_count)[:, None] * part_len + jnp.arange(part_len)[None]
    keep = row_pos[:, :, None] >= jnp.arange(block_len)[None, None]
    weights = jnp.where(keep[:, None, None], scores, 0.0).astype(jnp.bfloat16)
    in_block = jnp.einsum('ibhts,sbhv->itbhv', weights, v_blk, preferred_element_type=jnp.float32)
    in_block = in_block.reshape((block_len,) + in_block.shape[2:])
    block_total = within[-1]
    start_query = (q_wide * jnp.exp(within)).astype(jnp.bfloat16)
    end_key = (k_wide * jnp.exp(block_total[None] - within)).astype(jnp.bfloat16)
    added = jnp.einsum('sbhk,sbhv->bhkv', end_key, v_blk, preferred_element_type=jnp.float32)
    return (in_block, start_query, block_total, added)

def block_attention(query_all, key_all, value_all, decay_all, start_states):
    seq_len = query_all.shape[0]
    block_count = seq_len // BLOCK

    def to_blocks(tensor):
        return tensor.reshape((block_count, BLOCK) + tensor.shape[1:])

    def advance(states, inputs):
        in_block, start_query, block_total, added = block_terms(*inputs)
        from_state = jnp.einsum('tbhk,bhkv->tbhv', start_query.astype(jnp.float32), states, precision=highest)
        carried = jnp.exp(block_total)[..., None] * states + added
        return (carried, from_state + in_block)
    final_states, outputs = lax.scan(advance, start_states, (to_blocks(query_all), to_blocks(key_all), to_blocks(value_all), to_blocks(decay_all)))
    return (outputs.reshape((seq_len,) + outputs.shape[2:]), final_states)

def single_token(query, key_new, value_new, decay, states):
    query = query.astype(jnp.float32)
    key_new = key_new.astype(jnp.float32)
    value_new = value_new.astype(jnp.float32)
    from_state = jnp.einsum('bhk,bhkv->bhv', query * jnp.exp(decay), states, precision=highest)
    token_score = lax.optimization_barrier(jnp.sum(query * key_new, axis=-1, keepdims=True))
    outputs = from_state + token_score * value_new
    carried = jnp.exp(decay)[..., None] * states + key_new[..., None] * value_new[..., None, :]
    return (outputs, carried)

def reference(pieces, new_tokens, w_query, w_key, w_value, w_decay, decay_bias, norm_gain, head_gain, w_out, prompt_state, decode_state):
    query_p, key_p, value_p, decay_p = project_roles(rms_rows(pieces, norm_gain), w_query, w_key, w_value, w_decay, decay_bias)
    piece_att, prompt_out = block_attention(query_p, key_p, value_p, decay_p, prompt_state)
    query_d, key_d, value_d, decay_d = project_roles(rms_rows(new_tokens, norm_gain), w_query, w_key, w_value, w_decay, decay_bias)
    decode_att, decode_out = single_token(query_d, key_d, value_d, decay_d, decode_state)
    mixed_piece = jnp.dot(head_norm(piece_att, head_gain), w_out, preferred_element_type=jnp.float32).astype(jnp.bfloat16)
    mixed_decode = jnp.dot(head_norm(decode_att, head_gain), w_out, preferred_element_type=jnp.float32).astype(jnp.bfloat16)
    return (mixed_piece, mixed_decode, prompt_out, decode_out)
```

```python
import functools

import jax
import jax.numpy as jnp
from jax import lax
from jax.experimental import pallas as pl
from jax.experimental.pallas import tpu as pltpu
from jax.sharding import PartitionSpec as P

F32 = jnp.float32
BF16 = jnp.bfloat16
MESH = pl.DeviceIdType.MESH

DK = 128
DV = 256
EPS = 0.1
TAU = 16.0
SUB = 16
BLK = 64
HEADS = 4
PR = 2
OWN = 128
PAD = 16
RP = PR * OWN
ROWS = RP + PAD
KVN = 16
PH = PR * HEADS
TN = (((0,), (0,)), ((), ()))
NT = (((1,), (1,)), ((), ()))


def dot(a, b):
    return jnp.dot(a, b, preferred_element_type=F32)


def dotg(a, b, dims):
    return lax.dot_general(a, b, dims, preferred_element_type=F32)


def log_decay(x):
    return (jnp.minimum(x, 0.0) - jnp.log1p(jnp.exp(-jnp.abs(x)))) / TAU


def order_matrix():
    m = lax.broadcasted_iota(jnp.int32, (RP, RP), 0)
    n = lax.broadcasted_iota(jnp.int32, (RP, RP), 1)
    first = jnp.where(m < OWN, PR * m, PR * (m - OWN) + 1)
    return jnp.where(n == first, 1.0, 0.0).astype(BF16)


def attend_kernel(
    pieces, new_tokens, w_query, w_key, w_value, w_decay, bias, gain, head_gain, prompt_state, decode_state,
    own_out, peer_out, prompt_out, dec_key, dec_value, dec_decay,
    x3, nt, wq, wk, wv, wd, bias_v, gain_v, hg_v, ps, ds, xs, rows, qb, kb, vb, db, bb, st, tt, ttt, rs, rt, sb, inc, att,
    sqc, nrm, load_sem, row_sem, st_send, st_recv, tt_send, tt_recv, in_send, in_recv, nrm_sem,
):
    kv = lax.axis_index("kv")
    tp = lax.axis_index("tp")
    other = 1 - tp

    loads = [
        pltpu.make_async_copy(src, dst, load_sem.at[i])
        for i, (src, dst) in enumerate(
            [
                (pieces, x3), (new_tokens, nt), (gain, gain_v), (w_decay, wd), (w_key, wk), (w_value, wv),
                (bias, bias_v), (w_query, wq), (prompt_state, ps), (decode_state, ds), (head_gain, hg_v),
            ]
        )
    ]
    for copy in loads:
        copy.start()

    barrier = pltpu.get_barrier_semaphore()
    pl.semaphore_signal(barrier, inc=1, device_id={"tp": other}, device_id_type=MESH)
    for d in range(1, KVN):
        pl.semaphore_signal(barrier, inc=1, device_id={"kv": lax.rem(kv + d, KVN)}, device_id_type=MESH)

    order = order_matrix()
    for copy in loads[:3]:
        copy.wait()
    flat = x3[...].reshape(RP, x3.shape[-1])
    width = flat.shape[-1]
    step = 512
    squares = jnp.zeros((RP, 1), F32)
    for c in range(width // step):
        part = dot(order, flat[:, c * step : (c + 1) * step])
        xs[:, c * step : (c + 1) * step] = part
        squares += jnp.sum(part * part, axis=-1, keepdims=True)
    factor = lax.rsqrt(squares / width + EPS)
    for c in range(width // step):
        cols = slice(c * step, (c + 1) * step)
        rows[tp, :RP, cols] = (xs[:, cols] * factor * gain_v[:, cols]).astype(BF16)
    wide = nt[...].astype(F32)
    nt_factor = lax.rsqrt(jnp.sum(wide * wide, axis=-1, keepdims=True) / width + EPS)
    nt_rows = wide * nt_factor * gain_v[...]
    rows[tp, RP:, :] = jnp.concatenate([nt_rows, jnp.zeros((PAD - nt_rows.shape[0], width), F32)], axis=0).astype(BF16)

    pl.semaphore_wait(barrier, KVN)
    row_copy = pltpu.make_async_remote_copy(
        src_ref=rows.at[tp], dst_ref=rows.at[tp], send_sem=row_sem.at[0], recv_sem=row_sem.at[1],
        device_id={"tp": other}, device_id_type=MESH,
    )
    row_copy.start()

    def project(half, weights, out, kind):
        per = 2 * DK

        def tile(j, _):
            cols = pl.ds(pl.multiple_of(j * per, per), per)
            got = dot(rows[half], weights[:, cols])
            if kind == "v":
                out[j, half] = got.astype(BF16)
            else:
                for e in range(2):
                    part = got[:, e * DK : (e + 1) * DK]
                    if kind == "q":
                        part = (part * DK**-0.5).astype(BF16)
                    elif kind == "k":
                        part = part.astype(BF16)
                    else:
                        at = pl.multiple_of(tp * (HEADS * DK) + j * per + e * DK, DK)
                        part = log_decay(part + bias_v[:, pl.ds(at, DK)])
                    out[2 * j + e, half] = part
            return 0

        lax.fori_loop(0, weights.shape[1] // per, tile, 0)

    for i in (3, 4, 5, 6):
        loads[i].wait()
    project(tp, wd, db, "d")
    project(tp, wk, kb, "k")
    project(tp, wv, vb, "v")
    row_copy.wait()
    project(other, wd, db, "d")
    project(other, wk, kb, "k")
    project(other, wv, vb, "v")

    t_at = lax.broadcasted_iota(jnp.int32, (OWN, OWN), 0)
    s_at = lax.broadcasted_iota(jnp.int32, (OWN, OWN), 1)
    lower = jnp.where(t_at >= s_at, 1.0, 0.0).astype(BF16)
    lower2 = jnp.concatenate([lower, lower], axis=1)

    def sums(i, _):
        half, p = i // PR, i % PR
        at = pl.ds(pl.multiple_of(p * OWN, OWN), OWN)
        g = jnp.concatenate([db[h, half, at] for h in range(HEADS)], axis=1)
        hi = g.astype(BF16)
        lo = (g - hi.astype(F32)).astype(BF16)
        got = dot(lower2, jnp.concatenate([hi, lo], axis=0))
        for h in range(HEADS):
            bb[h, half, p] = got[:, h * DK : (h + 1) * DK]
        return 0

    lax.fori_loop(0, 2 * PR, sums, 0)

    tt[...] = jnp.zeros_like(tt)

    def add_state(p, _):
        at = pl.ds(pl.multiple_of(p * OWN, OWN), OWN)
        for h in range(HEADS):
            b0, b1 = bb[h, 0, p], bb[h, 1, p]
            t0, t1 = b0[OWN - 1 :], b1[OWN - 1 :]
            e0 = kb[h, 0, at].astype(F32) * jnp.exp((t0 - b0) + t1)
            e1 = kb[h, 1, at].astype(F32) * jnp.exp(t1 - b1)
            keys = jnp.concatenate([e0.astype(BF16), e1.astype(BF16)], axis=0)
            vals = jnp.concatenate([vb[h, 0, at], vb[h, 1, at]], axis=0)
            state = dotg(keys, vals, TN)
            st[:, p * HEADS + h] = state.reshape(KVN, DK // KVN, DV).astype(BF16)
            tt[pl.ds(p * HEADS + h, 1), :] = t0 + t1
        return 0

    lax.fori_loop(0, PR, add_state, 0)
    ttt[...] = tt[...].T.reshape(KVN, DK // KVN, DK)

    def state_copy(to, slot):
        return pltpu.make_async_remote_copy(
            src_ref=st.at[to], dst_ref=rs.at[slot], send_sem=st_send.at[to], recv_sem=st_recv.at[slot],
            device_id={"kv": to}, device_id_type=MESH,
        )

    def total_copy(to, slot):
        return pltpu.make_async_remote_copy(
            src_ref=ttt.at[to], dst_ref=rt.at[slot], send_sem=tt_send.at[to], recv_sem=tt_recv.at[slot],
            device_id={"kv": to}, device_id_type=MESH,
        )

    def back_copy(to, slot):
        return pltpu.make_async_remote_copy(
            src_ref=sb.at[to], dst_ref=inc.at[slot], send_sem=in_send.at[to], recv_sem=in_recv.at[slot],
            device_id={"kv": to}, device_id_type=MESH,
        )

    for d in range(1, KVN):
        to = lax.rem(kv + d, KVN)
        total_copy(to, kv).start()
        state_copy(to, kv).start()
    rs[kv] = st[kv]
    rt[kv] = ttt[kv]

    loads[7].wait()
    project(0, wq, qb, "q")
    project(1, wq, qb, "q")

    t_in = lax.broadcasted_iota(jnp.int32, (BLK, BLK), 0)
    s_in = lax.broadcasted_iota(jnp.int32, (BLK, BLK), 1)
    keep = t_in >= s_in

    def inside(i, _):
        p, h = i // HEADS, i % HEADS
        at = pl.ds(pl.multiple_of(p * OWN, OWN), OWN)
        ks = [kb[h, half, at].astype(F32) for half in range(2)]
        qs = [qb[h, half, at].astype(F32) for half in range(2)]
        bs = [bb[h, half, p] for half in range(2)]
        vs = [vb[h, half, at] for half in range(2)]
        m0, t0 = bs[0][BLK - 1 : BLK], bs[0][OWN - 1 :]
        m1 = bs[1][BLK - 1 : BLK]
        first = (ks[0][:BLK] * jnp.exp(m0 - bs[0][:BLK])).astype(BF16)
        state1 = dotg(first, vs[0][:BLK], TN)
        second = ks[0] * jnp.exp(t0 - bs[0])
        state2 = dotg(second.astype(BF16), vs[0], TN)
        third = jnp.concatenate(
            [(ks[0] * jnp.exp((t0 - bs[0]) + m1)).astype(BF16), (ks[1][:BLK] * jnp.exp(m1 - bs[1][:BLK])).astype(BF16)], axis=0
        )
        state3 = dotg(third, jnp.concatenate([vs[0], vs[1][:BLK]], axis=0), TN)
        starts = [None, state1, state2, state3]
        for blk in range(4):
            half, lo = blk // 2, (blk % 2) * BLK
            b = bs[half][lo : lo + BLK]
            q = qs[half][lo : lo + BLK]
            k = ks[half][lo : lo + BLK]
            v = vs[half][lo : lo + BLK]
            ref = [jnp.zeros((1, DK), F32) if lo == 0 else bs[half][lo - 1 : lo]]
            for n in range(1, BLK // SUB):
                ref.append(b[n * SUB - 1 : n * SUB])
            zero = jnp.zeros((SUB, DK), BF16)
            q_rows, k_cols = [], []
            for n in range(BLK // SUB):
                end = (n + 1) * SUB
                near_q = (q[n * SUB : end] * jnp.exp(b[n * SUB : end] - ref[n])).astype(BF16)
                near_k = (k[:end] * jnp.exp(ref[n] - b[:end])).astype(BF16)
                q_rows.append(jnp.concatenate([near_q if m == n else zero for m in range(BLK // SUB)], axis=1))
                k_cols.append(jnp.concatenate([near_k] + [zero] * (BLK // SUB - 1 - n), axis=0))
            scores = dotg(jnp.concatenate(q_rows, axis=0), jnp.concatenate(k_cols, axis=1), NT)
            weights = jnp.where(keep, scores, 0.0).astype(BF16)
            if blk == 0:
                out = dot(weights, v)
            else:
                start_q = (q * jnp.exp(b - ref[0])).astype(BF16)
                out = dot(
                    jnp.concatenate([start_q, weights], axis=1),
                    jnp.concatenate([starts[blk].astype(BF16), v], axis=0),
                )
            att[i, half, lo : lo + BLK] = out
        sqc[i, 0] = (qs[0] * jnp.exp(bs[0])).astype(BF16)
        sqc[i, 1] = (qs[1] * jnp.exp(bs[1] + t0)).astype(BF16)
        return 0

    lax.fori_loop(0, PH, inside, 0)

    for i in (8, 9, 10):
        loads[i].wait()

    def normed(out, h):
        scale = lax.rsqrt(jnp.sum(out * out, axis=-1, keepdims=True) / DV + EPS)
        gain_at = pl.multiple_of(tp * (HEADS * DV) + h * DV, DV)
        return (out * scale * hg_v[:, pl.ds(gain_at, DV)]).astype(BF16)

    tt[...] = jnp.zeros_like(tt)
    each = 2
    for half in range(2):
        for h in range(HEADS):
            q = qb[h, half, RP:].astype(F32)
            k = kb[h, half, RP:].astype(F32)
            v = vb[h, half, RP:].astype(F32)
            eg = jnp.exp(db[h, half, RP:])
            eq = (q * eg).astype(BF16)
            row = lax.broadcasted_iota(jnp.int32, (PAD, 1), 0)
            out = jnp.sum(q * k, axis=-1, keepdims=True) * v
            for r in range(each):
                from_state = dot(eq, ds[each * half + r, h].astype(BF16))
                out = out + jnp.where(row == r, from_state, 0.0)
                tt[pl.ds((each * half + r) * HEADS + h, 1), :] = eg[r : r + 1]
            nrm[half, RP:, h * DV : (h + 1) * DV] = normed(out, h)
            dec_key[half, h] = kb[h, half, RP:]
            dec_value[half, h] = vb[h, half, RP:]
    dec_decay[...] = tt[...].T

    def scan_step(i, state):
        @pl.when(i != kv)
        def _():
            total_copy(i, i).wait_recv()
            state_copy(i, i).wait_recv()

        sb[i] = state.astype(BF16)

        @pl.when(i != kv)
        def _():
            back_copy(i, kv).start()

        decay = jnp.exp(rt[i])
        return jnp.stack(
            [decay[:, n : n + 1] * state[n] + rs[i, n].astype(F32) for n in range(PH)], axis=0
        )

    prompt_out[...] = lax.fori_loop(0, KVN, scan_step, ps[...])
    inc[kv] = sb[kv]
    for d in range(1, KVN):
        frm = lax.rem(kv + d, KVN)
        back_copy(frm, frm).wait_recv()

    def finish(i, _):
        p, h = i // HEADS, i % HEADS
        incoming = inc[:, i].astype(F32).reshape(DK, DV).astype(BF16)
        at = pl.ds(pl.multiple_of(p * OWN, OWN), OWN)
        cols = pl.ds(pl.multiple_of(h * DV, DV), DV)
        for half in range(2):
            out = att[i, half] + dot(sqc[i, half], incoming)
            nrm[half, at, cols] = normed(out, h)
        return 0

    lax.fori_loop(0, PH, finish, 0)

    nrm_copy = pltpu.make_async_remote_copy(
        src_ref=nrm.at[other], dst_ref=peer_out, send_sem=nrm_sem.at[0], recv_sem=nrm_sem.at[1],
        device_id={"tp": other}, device_id_type=MESH,
    )
    nrm_copy.start()
    own_out[...] = nrm[tp]
    nrm_copy.wait()
    for d in range(1, KVN):
        to = lax.rem(kv + d, KVN)
        total_copy(to, kv).wait_send()
        state_copy(to, kv).wait_send()
        back_copy(to, kv).wait_send()


def finish_kernel(own, peer, w_out, prompt_in, dec_key, dec_value, dec_decay, decode_state, mixed, mixed_dec, prompt_out, dec_out, lhs):
    tp = lax.axis_index("tp")
    n = pl.program_id(0)
    half_width = own.shape[-1]

    @pl.when(n == 0)
    def _():
        order = order_matrix()
        prompt_out[...] = prompt_in[...]
        for src, at in ((own, tp), (peer, 1 - tp)):
            cols = pl.ds(pl.multiple_of(at * half_width, half_width), half_width)
            lhs[:RP, cols] = dotg(order, src[:RP], TN).astype(BF16)
            lhs[RP:, cols] = src[RP:]

    got = dot(lhs[...], w_out[...]).astype(BF16)
    mixed[...] = got[:RP].reshape(OWN, PR, got.shape[-1])
    mixed_dec[...] = got[RP : RP + 2]
    row = lax.broadcasted_iota(jnp.int32, (PAD, 1), 0)
    for e in range(2):
        idx = 2 * n + e
        token, h = idx // HEADS, idx % HEADS
        half, r = token // 2, token % 2
        key = jnp.where(row == r, dec_key[half, h].astype(F32), 0.0).astype(BF16)
        fresh = dotg(key, dec_value[half, h], TN)
        lane = lax.broadcasted_iota(jnp.int32, (1, DK), 1)
        decay = jnp.sum(jnp.where(lane == idx, dec_decay[...], 0.0), axis=-1, keepdims=True)
        dec_out[e] = decay * decode_state[e] + fresh


def on_device(
    pieces, new_tokens, w_query, w_key, w_value, w_decay, decay_bias, norm_gain, head_gain, w_out, prompt_state, decode_state
):
    width = pieces.shape[-1]
    any_spec = pl.BlockSpec(memory_space=pl.ANY)
    vmem = pl.BlockSpec(memory_space=pltpu.VMEM)
    dma = pltpu.SemaphoreType.DMA
    row_k = DK // KVN
    own, peer, prompt_new, dec_key, dec_value, dec_decay = pl.pallas_call(
        attend_kernel,
        name="attend",
        out_shape=(
            jax.ShapeDtypeStruct((ROWS, HEADS * DV), BF16),
            jax.ShapeDtypeStruct((ROWS, HEADS * DV), BF16),
            jax.ShapeDtypeStruct((PH, row_k, DV), F32),
            jax.ShapeDtypeStruct((2, HEADS, PAD, DK), BF16),
            jax.ShapeDtypeStruct((2, HEADS, PAD, DV), BF16),
            jax.ShapeDtypeStruct((DK, DK), F32),
        ),
        in_specs=[any_spec] * 11,
        out_specs=(vmem,) * 6,
        scratch_shapes=[
            pltpu.VMEM((OWN, PR, width), BF16),
            pltpu.VMEM((2, width), BF16),
            pltpu.VMEM((width, HEADS * DK), BF16),
            pltpu.VMEM((width, HEADS * DK), BF16),
            pltpu.VMEM((width, HEADS * DV), BF16),
            pltpu.VMEM((width, HEADS * DK), BF16),
            pltpu.VMEM((1, 2 * HEADS * DK), F32),
            pltpu.VMEM((1, width), F32),
            pltpu.VMEM((1, width), F32),
            pltpu.VMEM((PH, row_k, DV), F32),
            pltpu.VMEM((4, HEADS, DK, DV), F32),
            pltpu.VMEM((RP, width), F32),
            pltpu.VMEM((2, ROWS, width), BF16),
            pltpu.VMEM((HEADS, 2, ROWS, DK), BF16),
            pltpu.VMEM((HEADS, 2, ROWS, DK), BF16),
            pltpu.VMEM((HEADS, 2, ROWS, DV), BF16),
            pltpu.VMEM((HEADS, 2, ROWS, DK), F32),
            pltpu.VMEM((HEADS, 2, PR, OWN, DK), F32),
            pltpu.VMEM((KVN, PH, row_k, DV), BF16),
            pltpu.VMEM((DK, DK), F32),
            pltpu.VMEM((KVN, row_k, DK), F32),
            pltpu.VMEM((KVN, PH, row_k, DV), BF16),
            pltpu.VMEM((KVN, row_k, DK), F32),
            pltpu.VMEM((KVN, PH, row_k, DV), BF16),
            pltpu.VMEM((KVN, PH, row_k, DV), BF16),
            pltpu.VMEM((PH, 2, OWN, DV), F32),
            pltpu.VMEM((PH, 2, OWN, DK), BF16),
            pltpu.VMEM((2, ROWS, HEADS * DV), BF16),
            dma((11,)),
            dma((2,)),
            dma((KVN,)),
            dma((KVN,)),
            dma((KVN,)),
            dma((KVN,)),
            dma((KVN,)),
            dma((KVN,)),
            dma((2,)),
        ],
        compiler_params=pltpu.CompilerParams(collective_id=0, has_side_effects=True, vmem_limit_bytes=44 * 1024 * 1024),
    )(
        pieces, new_tokens, w_query, w_key, w_value, w_decay, decay_bias.reshape(1, -1), norm_gain.reshape(1, -1),
        head_gain.reshape(1, -1), prompt_state.reshape(PH, row_k, DV), decode_state,
    )
    steps = 8
    tile = width // steps
    full = lambda *shape: pl.BlockSpec(shape, lambda n: (0,) * len(shape))
    mixed, mixed_dec, prompt_out, dec_out = pl.pallas_call(
        finish_kernel,
        name="finish",
        grid=(steps,),
        out_shape=(
            jax.ShapeDtypeStruct((OWN, PR, width), BF16),
            jax.ShapeDtypeStruct((2, width), BF16),
            jax.ShapeDtypeStruct((PH, row_k, DV), F32),
            jax.ShapeDtypeStruct((4 * HEADS, DK, DV), F32),
        ),
        in_specs=[
            full(ROWS, HEADS * DV),
            full(ROWS, HEADS * DV),
            pl.BlockSpec((width, tile), lambda n: (0, n)),
            full(PH, row_k, DV),
            full(2, HEADS, PAD, DK),
            full(2, HEADS, PAD, DV),
            full(DK, DK),
            pl.BlockSpec((2, DK, DV), lambda n: (n, 0, 0)),
        ],
        out_specs=(
            pl.BlockSpec((OWN, PR, tile), lambda n: (0, 0, n)),
            pl.BlockSpec((2, tile), lambda n: (0, n)),
            full(PH, row_k, DV),
            pl.BlockSpec((2, DK, DV), lambda n: (n, 0, 0)),
        ),
        scratch_shapes=[pltpu.VMEM((ROWS, width), BF16)],
        compiler_params=pltpu.CompilerParams(dimension_semantics=("arbitrary",), vmem_limit_bytes=32 * 1024 * 1024),
    )(own, peer, w_out, prompt_new, dec_key, dec_value, dec_decay, decode_state.reshape(4 * HEADS, DK, DV))
    return (
        mixed,
        mixed_dec,
        prompt_out.reshape(prompt_state.shape),
        dec_out.reshape(decode_state.shape),
    )


def solution(mesh):
    kv_tp, dp_kv_tp = ("kv", "tp"), ("dp", "kv", "tp")
    return jax.shard_map(
        on_device,
        mesh=mesh,
        in_specs=(
            P(kv_tp, "dp", None),
            P(dp_kv_tp, None),
            P(None, "tp"),
            P(None, "tp"),
            P(None, "tp"),
            P(None, "tp"),
            P(),
            P(),
            P(),
            P(),
            P("dp", "tp", "kv", None),
            P(("dp", "kv"), "tp", None, None),
        ),
        out_specs=(
            P(kv_tp, "dp", None),
            P(dp_kv_tp, None),
            P("dp", "tp", "kv", None),
            P(("dp", "kv"), "tp", None, None),
        ),
        check_vma=False,
    )
```

```python
import functools

import jax
import jax.numpy as jnp
from jax import lax
from jax.experimental import pallas as pl
from jax.experimental.pallas import tpu as pltpu
from jax.sharding import PartitionSpec as P

F32 = jnp.float32
BF16 = jnp.bfloat16
MESH = pl.DeviceIdType.MESH

DK = 128
DV = 256
EPS = 0.1
TAU = 16.0
SUB = 16
BLK = 64
HEADS = 4
PR = 2
OWN = 128
PAD = 16
RP = PR * OWN
ROWS = RP + PAD
KVN = 16
PH = PR * HEADS
TN = (((0,), (0,)), ((), ()))
NT = (((1,), (1,)), ((), ()))


def dot(a, b):
    return jnp.dot(a, b, preferred_element_type=F32)


def dotg(a, b, dims):
    return lax.dot_general(a, b, dims, preferred_element_type=F32)


def log_decay(x):
    return (jnp.minimum(x, 0.0) - jnp.log1p(jnp.exp(-jnp.abs(x)))) / TAU


def order_matrix():
    m = lax.broadcasted_iota(jnp.int32, (RP, RP), 0)
    n = lax.broadcasted_iota(jnp.int32, (RP, RP), 1)
    first = jnp.where(m < OWN, PR * m, PR * (m - OWN) + 1)
    return jnp.where(n == first, 1.0, 0.0).astype(BF16)


def attend_kernel(
    pieces, new_tokens, w_query, w_key, w_value, w_decay, bias, gain, head_gain, prompt_state, decode_state,
    own_out, peer_out, prompt_out, dec_new,
    x3, nt, wq, wk, wv, wd, bias_v, gain_v, hg_v, ps, ds, xs, rows, qb, kb, vb, db, bb, st, tt, ttt, rs, rt, sb, inc, att,
    sqc, nrm, load_sem, row_sem, st_send, st_recv, tt_send, tt_recv, in_send, in_recv, nrm_sem,
):
    kv = lax.axis_index("kv")
    tp = lax.axis_index("tp")
    other = 1 - tp

    loads = [
        pltpu.make_async_copy(src, dst, load_sem.at[i])
        for i, (src, dst) in enumerate(
            [
                (pieces, x3), (new_tokens, nt), (gain, gain_v), (w_decay, wd), (w_key, wk), (w_value, wv),
                (bias, bias_v), (w_query, wq), (prompt_state, ps), (decode_state, ds), (head_gain, hg_v),
            ]
        )
    ]
    for copy in loads:
        copy.start()

    barrier = pltpu.get_barrier_semaphore()
    pl.semaphore_signal(barrier, inc=1, device_id={"tp": other}, device_id_type=MESH)
    for d in range(1, KVN):
        pl.semaphore_signal(barrier, inc=1, device_id={"kv": lax.rem(kv + d, KVN)}, device_id_type=MESH)

    order = order_matrix()
    for copy in loads[:3]:
        copy.wait()
    flat = x3[...].reshape(RP, x3.shape[-1])
    width = flat.shape[-1]
    step = 512
    squares = jnp.zeros((RP, 1), F32)
    for c in range(width // step):
        part = dot(order, flat[:, c * step : (c + 1) * step])
        xs[:, c * step : (c + 1) * step] = part
        squares += jnp.sum(part * part, axis=-1, keepdims=True)
    factor = lax.rsqrt(squares / width + EPS)
    for c in range(width // step):
        cols = slice(c * step, (c + 1) * step)
        rows[tp, :RP, cols] = (xs[:, cols] * factor * gain_v[:, cols]).astype(BF16)
    wide = nt[...].astype(F32)
    nt_factor = lax.rsqrt(jnp.sum(wide * wide, axis=-1, keepdims=True) / width + EPS)
    nt_rows = wide * nt_factor * gain_v[...]
    rows[tp, RP:, :] = jnp.concatenate([nt_rows, jnp.zeros((PAD - nt_rows.shape[0], width), F32)], axis=0).astype(BF16)

    pl.semaphore_wait(barrier, KVN)
    row_copy = pltpu.make_async_remote_copy(
        src_ref=rows.at[tp], dst_ref=rows.at[tp], send_sem=row_sem.at[0], recv_sem=row_sem.at[1],
        device_id={"tp": other}, device_id_type=MESH,
    )
    row_copy.start()

    def project(half, weights, out, kind):
        per = 2 * DK

        def tile(j, _):
            cols = pl.ds(pl.multiple_of(j * per, per), per)
            got = dot(rows[half], weights[:, cols])
            if kind == "v":
                out[j, half] = got.astype(BF16)
            else:
                for e in range(2):
                    part = got[:, e * DK : (e + 1) * DK]
                    if kind == "q":
                        part = (part * DK**-0.5).astype(BF16)
                    elif kind == "k":
                        part = part.astype(BF16)
                    else:
                        at = pl.multiple_of(tp * (HEADS * DK) + j * per + e * DK, DK)
                        part = log_decay(part + bias_v[:, pl.ds(at, DK)])
                    out[2 * j + e, half] = part
            return 0

        lax.fori_loop(0, weights.shape[1] // per, tile, 0)

    for i in (3, 4, 5, 6):
        loads[i].wait()
    project(tp, wd, db, "d")
    project(tp, wk, kb, "k")
    project(tp, wv, vb, "v")
    row_copy.wait()
    project(other, wd, db, "d")
    project(other, wk, kb, "k")
    project(other, wv, vb, "v")

    t_at = lax.broadcasted_iota(jnp.int32, (OWN, OWN), 0)
    s_at = lax.broadcasted_iota(jnp.int32, (OWN, OWN), 1)
    lower = jnp.where(t_at >= s_at, 1.0, 0.0).astype(BF16)
    lower2 = jnp.concatenate([lower, lower], axis=1)

    def sums(i, _):
        half, p = i // PR, i % PR
        at = pl.ds(pl.multiple_of(p * OWN, OWN), OWN)
        g = jnp.concatenate([db[h, half, at] for h in range(HEADS)], axis=1)
        hi = g.astype(BF16)
        lo = (g - hi.astype(F32)).astype(BF16)
        got = dot(lower2, jnp.concatenate([hi, lo], axis=0))
        for h in range(HEADS):
            bb[h, half, p] = got[:, h * DK : (h + 1) * DK]
        return 0

    lax.fori_loop(0, 2 * PR, sums, 0)

    tt[...] = jnp.zeros_like(tt)

    def add_state(p, _):
        at = pl.ds(pl.multiple_of(p * OWN, OWN), OWN)
        for h in range(HEADS):
            b0, b1 = bb[h, 0, p], bb[h, 1, p]
            t0, t1 = b0[OWN - 1 :], b1[OWN - 1 :]
            e0 = kb[h, 0, at].astype(F32) * jnp.exp((t0 - b0) + t1)
            e1 = kb[h, 1, at].astype(F32) * jnp.exp(t1 - b1)
            keys = jnp.concatenate([e0.astype(BF16), e1.astype(BF16)], axis=0)
            vals = jnp.concatenate([vb[h, 0, at], vb[h, 1, at]], axis=0)
            state = dotg(keys, vals, TN)
            st[:, p * HEADS + h] = state.reshape(KVN, DK // KVN, DV).astype(BF16)
            tt[pl.ds(p * HEADS + h, 1), :] = t0 + t1
        return 0

    lax.fori_loop(0, PR, add_state, 0)
    ttt[...] = tt[...].T.reshape(KVN, DK // KVN, DK)

    def state_copy(to, slot):
        return pltpu.make_async_remote_copy(
            src_ref=st.at[to], dst_ref=rs.at[slot], send_sem=st_send.at[to], recv_sem=st_recv.at[slot],
            device_id={"kv": to}, device_id_type=MESH,
        )

    def total_copy(to, slot):
        return pltpu.make_async_remote_copy(
            src_ref=ttt.at[to], dst_ref=rt.at[slot], send_sem=tt_send.at[to], recv_sem=tt_recv.at[slot],
            device_id={"kv": to}, device_id_type=MESH,
        )

    def back_copy(to, slot):
        return pltpu.make_async_remote_copy(
            src_ref=sb.at[to], dst_ref=inc.at[slot], send_sem=in_send.at[to], recv_sem=in_recv.at[slot],
            device_id={"kv": to}, device_id_type=MESH,
        )

    for d in range(1, KVN):
        to = lax.rem(kv + d, KVN)
        total_copy(to, kv).start()
        state_copy(to, kv).start()
    rs[kv] = st[kv]
    rt[kv] = ttt[kv]

    loads[7].wait()
    project(0, wq, qb, "q")
    project(1, wq, qb, "q")

    t_in = lax.broadcasted_iota(jnp.int32, (BLK, BLK), 0)
    s_in = lax.broadcasted_iota(jnp.int32, (BLK, BLK), 1)
    keep = t_in >= s_in

    def inside(i, _):
        p, h = i // HEADS, i % HEADS
        at = pl.ds(pl.multiple_of(p * OWN, OWN), OWN)
        ks = [kb[h, half, at].astype(F32) for half in range(2)]
        qs = [qb[h, half, at].astype(F32) for half in range(2)]
        bs = [bb[h, half, p] for half in range(2)]
        vs = [vb[h, half, at] for half in range(2)]
        m0, t0 = bs[0][BLK - 1 : BLK], bs[0][OWN - 1 :]
        m1 = bs[1][BLK - 1 : BLK]
        first = (ks[0][:BLK] * jnp.exp(m0 - bs[0][:BLK])).astype(BF16)
        state1 = dotg(first, vs[0][:BLK], TN)
        second = ks[0] * jnp.exp(t0 - bs[0])
        state2 = dotg(second.astype(BF16), vs[0], TN)
        third = jnp.concatenate(
            [(ks[0] * jnp.exp((t0 - bs[0]) + m1)).astype(BF16), (ks[1][:BLK] * jnp.exp(m1 - bs[1][:BLK])).astype(BF16)], axis=0
        )
        state3 = dotg(third, jnp.concatenate([vs[0], vs[1][:BLK]], axis=0), TN)
        starts = [None, state1, state2, state3]
        for blk in range(4):
            half, lo = blk // 2, (blk % 2) * BLK
            b = bs[half][lo : lo + BLK]
            q = qs[half][lo : lo + BLK]
            k = ks[half][lo : lo + BLK]
            v = vs[half][lo : lo + BLK]
            ref = [jnp.zeros((1, DK), F32) if lo == 0 else bs[half][lo - 1 : lo]]
            for n in range(1, BLK // SUB):
                ref.append(b[n * SUB - 1 : n * SUB])
            zero = jnp.zeros((SUB, DK), BF16)
            q_rows, k_cols = [], []
            for n in range(BLK // SUB):
                end = (n + 1) * SUB
                near_q = (q[n * SUB : end] * jnp.exp(b[n * SUB : end] - ref[n])).astype(BF16)
                near_k = (k[:end] * jnp.exp(ref[n] - b[:end])).astype(BF16)
                q_rows.append(jnp.concatenate([near_q if m == n else zero for m in range(BLK // SUB)], axis=1))
                k_cols.append(jnp.concatenate([near_k] + [zero] * (BLK // SUB - 1 - n), axis=0))
            scores = dotg(jnp.concatenate(q_rows, axis=0), jnp.concatenate(k_cols, axis=1), NT)
            weights = jnp.where(keep, scores, 0.0).astype(BF16)
            if blk == 0:
                out = dot(weights, v)
            else:
                start_q = (q * jnp.exp(b - ref[0])).astype(BF16)
                out = dot(
                    jnp.concatenate([start_q, weights], axis=1),
                    jnp.concatenate([starts[blk].astype(BF16), v], axis=0),
                )
            att[i, half, lo : lo + BLK] = out
        sqc[i, 0] = (qs[0] * jnp.exp(bs[0])).astype(BF16)
        sqc[i, 1] = (qs[1] * jnp.exp(bs[1] + t0)).astype(BF16)
        return 0

    lax.fori_loop(0, PH, inside, 0)

    for i in (8, 9, 10):
        loads[i].wait()

    def normed(out, h):
        scale = lax.rsqrt(jnp.sum(out * out, axis=-1, keepdims=True) / DV + EPS)
        gain_at = pl.multiple_of(tp * (HEADS * DV) + h * DV, DV)
        return (out * scale * hg_v[:, pl.ds(gain_at, DV)]).astype(BF16)

    tt[...] = jnp.zeros_like(tt)
    each = 2
    for half in range(2):
        for h in range(HEADS):
            q = qb[h, half, RP:].astype(F32)
            k = kb[h, half, RP:].astype(F32)
            v = vb[h, half, RP:].astype(F32)
            eg = jnp.exp(db[h, half, RP:])
            eq = (q * eg).astype(BF16)
            row = lax.broadcasted_iota(jnp.int32, (PAD, 1), 0)
            out = jnp.sum(q * k, axis=-1, keepdims=True) * v
            for r in range(each):
                from_state = dot(eq, ds[each * half + r, h].astype(BF16))
                out = out + jnp.where(row == r, from_state, 0.0)
                tt[pl.ds((each * half + r) * HEADS + h, 1), :] = eg[r : r + 1]
            nrm[half, RP:, h * DV : (h + 1) * DV] = normed(out, h)
    tt[...] = tt[...].T
    for half in range(2):
        for h in range(HEADS):
            for r in range(each):
                token = each * half + r
                key = jnp.where(row == r, kb[h, half, RP:].astype(F32), 0.0).astype(BF16)
                fresh = dotg(key, vb[h, half, RP:], TN)
                idx = token * HEADS + h
                dec_new[token, h] = tt[:, idx : idx + 1] * ds[token, h] + fresh

    def scan_step(i, state):
        @pl.when(i != kv)
        def _():
            total_copy(i, i).wait_recv()
            state_copy(i, i).wait_recv()

        sb[i] = state.astype(BF16)

        @pl.when(i != kv)
        def _():
            back_copy(i, kv).start()

        decay = jnp.exp(rt[i])
        return jnp.stack(
            [decay[:, n : n + 1] * state[n] + rs[i, n].astype(F32) for n in range(PH)], axis=0
        )

    prompt_out[...] = lax.fori_loop(0, KVN, scan_step, ps[...])
    inc[kv] = sb[kv]
    for d in range(1, KVN):
        frm = lax.rem(kv + d, KVN)
        back_copy(frm, frm).wait_recv()

    def finish(i, _):
        p, h = i // HEADS, i % HEADS
        incoming = inc[:, i].astype(F32).reshape(DK, DV).astype(BF16)
        at = pl.ds(pl.multiple_of(p * OWN, OWN), OWN)
        cols = pl.ds(pl.multiple_of(h * DV, DV), DV)
        for half in range(2):
            out = att[i, half] + dot(sqc[i, half], incoming)
            nrm[half, at, cols] = normed(out, h)
        return 0

    lax.fori_loop(0, PH, finish, 0)

    nrm_copy = pltpu.make_async_remote_copy(
        src_ref=nrm.at[other], dst_ref=peer_out, send_sem=nrm_sem.at[0], recv_sem=nrm_sem.at[1],
        device_id={"tp": other}, device_id_type=MESH,
    )
    nrm_copy.start()
    own_out[...] = nrm[tp]
    nrm_copy.wait()
    for d in range(1, KVN):
        to = lax.rem(kv + d, KVN)
        total_copy(to, kv).wait_send()
        state_copy(to, kv).wait_send()
        back_copy(to, kv).wait_send()


def finish_kernel(own, peer, w_out, prompt_in, dec_in, mixed, mixed_dec, prompt_out, dec_out, lhs, out3, out2, sem, tile_sem):
    tp = lax.axis_index("tp")
    half_width = own.shape[-1]
    width = w_out.shape[-1]
    copies = [pltpu.make_async_copy(dec_in, dec_out, sem.at[0]), pltpu.make_async_copy(prompt_in, prompt_out, sem.at[1])]
    for copy in copies:
        copy.start()
    order = order_matrix()
    for src, at in ((own, tp), (peer, 1 - tp)):
        cols = pl.ds(pl.multiple_of(at * half_width, half_width), half_width)
        lhs[:RP, cols] = dotg(order, src[:RP], TN).astype(BF16)
        lhs[RP:, cols] = src[RP:]
    tile = 256

    def out_copy(n):
        cols = pl.ds(pl.multiple_of(n * tile, tile), tile)
        return pltpu.make_async_copy(out3.at[:, :, cols], mixed.at[:, :, cols], tile_sem.at[n])

    def body(n, _):
        cols = pl.ds(pl.multiple_of(n * tile, tile), tile)
        got = dot(lhs[...], w_out[:, cols]).astype(BF16)
        out3[:, :, cols] = got[:RP].reshape(OWN, PR, tile)
        out2[:, cols] = got[RP : RP + 2]
        out_copy(n).start()
        return 0

    lax.fori_loop(0, width // tile, body, 0)
    last = pltpu.make_async_copy(out2, mixed_dec, sem.at[2])
    last.start()
    for n in range(width // tile):
        out_copy(n).wait()
    last.wait()
    for copy in copies:
        copy.wait()


def on_device(
    pieces, new_tokens, w_query, w_key, w_value, w_decay, decay_bias, norm_gain, head_gain, w_out, prompt_state, decode_state
):
    width = pieces.shape[-1]
    vmem = pl.BlockSpec(memory_space=pltpu.VMEM)
    dma = pltpu.SemaphoreType.DMA
    row_k = DK // KVN
    hbm = pl.BlockSpec(memory_space=pltpu.HBM)
    own, peer, prompt_new, dec_new = pl.pallas_call(
        attend_kernel,
        name="attend",
        out_shape=(
            jax.ShapeDtypeStruct((ROWS, HEADS * DV), BF16),
            jax.ShapeDtypeStruct((ROWS, HEADS * DV), BF16),
            jax.ShapeDtypeStruct((PH, row_k, DV), F32),
            jax.ShapeDtypeStruct((4, HEADS, DK, DV), F32),
        ),
        in_specs=[hbm] * 11,
        out_specs=(vmem,) * 4,
        scratch_shapes=[
            pltpu.VMEM((OWN, PR, width), BF16),
            pltpu.VMEM((2, width), BF16),
            pltpu.VMEM((width, HEADS * DK), BF16),
            pltpu.VMEM((width, HEADS * DK), BF16),
            pltpu.VMEM((width, HEADS * DV), BF16),
            pltpu.VMEM((width, HEADS * DK), BF16),
            pltpu.VMEM((1, 2 * HEADS * DK), F32),
            pltpu.VMEM((1, width), F32),
            pltpu.VMEM((1, width), F32),
            pltpu.VMEM((PH, row_k, DV), F32),
            pltpu.VMEM((4, HEADS, DK, DV), F32),
            pltpu.VMEM((RP, width), F32),
            pltpu.VMEM((2, ROWS, width), BF16),
            pltpu.VMEM((HEADS, 2, ROWS, DK), BF16),
            pltpu.VMEM((HEADS, 2, ROWS, DK), BF16),
            pltpu.VMEM((HEADS, 2, ROWS, DV), BF16),
            pltpu.VMEM((HEADS, 2, ROWS, DK), F32),
            pltpu.VMEM((HEADS, 2, PR, OWN, DK), F32),
            pltpu.VMEM((KVN, PH, row_k, DV), BF16),
            pltpu.VMEM((DK, DK), F32),
            pltpu.VMEM((KVN, row_k, DK), F32),
            pltpu.VMEM((KVN, PH, row_k, DV), BF16),
            pltpu.VMEM((KVN, row_k, DK), F32),
            pltpu.VMEM((KVN, PH, row_k, DV), BF16),
            pltpu.VMEM((KVN, PH, row_k, DV), BF16),
            pltpu.VMEM((PH, 2, OWN, DV), F32),
            pltpu.VMEM((PH, 2, OWN, DK), BF16),
            pltpu.VMEM((2, ROWS, HEADS * DV), BF16),
            dma((11,)),
            dma((2,)),
            dma((KVN,)),
            dma((KVN,)),
            dma((KVN,)),
            dma((KVN,)),
            dma((KVN,)),
            dma((KVN,)),
            dma((2,)),
        ],
        compiler_params=pltpu.CompilerParams(collective_id=0, has_side_effects=True, vmem_limit_bytes=44 * 1024 * 1024),
    )(
        *(
            pltpu.with_memory_space_constraint(a, pltpu.HBM)
            for a in (
                pieces, new_tokens, w_query, w_key, w_value, w_decay, decay_bias.reshape(1, -1), norm_gain.reshape(1, -1),
                head_gain.reshape(1, -1), prompt_state.reshape(PH, row_k, DV), decode_state,
            )
        )
    )
    mixed, mixed_dec, prompt_out, dec_out = pl.pallas_call(
        finish_kernel,
        name="finish",
        out_shape=(
            jax.ShapeDtypeStruct((OWN, PR, width), BF16),
            jax.ShapeDtypeStruct((2, width), BF16),
            jax.ShapeDtypeStruct((PH, row_k, DV), F32),
            jax.ShapeDtypeStruct((4, HEADS, DK, DV), F32),
        ),
        in_specs=[vmem] * 5,
        out_specs=(hbm,) * 4,
        scratch_shapes=[
            pltpu.VMEM((ROWS, width), BF16),
            pltpu.VMEM((OWN, PR, width), BF16),
            pltpu.VMEM((2, width), BF16),
            dma((3,)),
            dma((width // 256,)),
        ],
        compiler_params=pltpu.CompilerParams(vmem_limit_bytes=32 * 1024 * 1024),
    )(own, peer, w_out, prompt_new, dec_new)
    return (
        mixed,
        mixed_dec,
        prompt_out.reshape(prompt_state.shape),
        dec_out,
    )


def solution(mesh):
    kv_tp, dp_kv_tp = ("kv", "tp"), ("dp", "kv", "tp")
    return jax.shard_map(
        on_device,
        mesh=mesh,
        in_specs=(
            P(kv_tp, "dp", None),
            P(dp_kv_tp, None),
            P(None, "tp"),
            P(None, "tp"),
            P(None, "tp"),
            P(None, "tp"),
            P(),
            P(),
            P(),
            P(),
            P("dp", "tp", "kv", None),
            P(("dp", "kv"), "tp", None, None),
        ),
        out_specs=(
            P(kv_tp, "dp", None),
            P(dp_kv_tp, None),
            P("dp", "tp", "kv", None),
            P(("dp", "kv"), "tp", None, None),
        ),
        check_vma=False,
    )
```

```python
import functools

import jax
import jax.numpy as jnp
from jax import lax
from jax.experimental import pallas as pl
from jax.experimental.pallas import tpu as pltpu
from jax.sharding import PartitionSpec as P

F32 = jnp.float32
BF16 = jnp.bfloat16
MESH = pl.DeviceIdType.MESH

DK = 128
DV = 256
EPS = 0.1
TAU = 16.0
SUB = 16
BLK = 64
HEADS = 4
PR = 2
OWN = 128
PAD = 16
RP = PR * OWN
ROWS = RP + PAD
KVN = 16
SIDE = 4
ROW_K = DK // KVN
PH = PR * HEADS
TN = (((0,), (0,)), ((), ()))
NT = (((1,), (1,)), ((), ()))


def dot(a, b):
    return jnp.dot(a, b, preferred_element_type=F32)


def dotg(a, b, dims):
    return lax.dot_general(a, b, dims, preferred_element_type=F32)


def log_decay(x):
    return (jnp.minimum(x, 0.0) - jnp.log1p(jnp.exp(-jnp.abs(x)))) / TAU


def order_matrix():
    m = lax.broadcasted_iota(jnp.int32, (RP, RP), 0)
    n = lax.broadcasted_iota(jnp.int32, (RP, RP), 1)
    first = jnp.where(m < OWN, PR * m, PR * (m - OWN) + 1)
    return jnp.where(n == first, 1.0, 0.0).astype(BF16)


def by_distance():
    offsets = [(dz, dy) for dz in range(SIDE) for dy in range(SIDE) if dz or dy]
    return sorted(offsets, key=lambda o: -min(o[0], SIDE - o[0]) - min(o[1], SIDE - o[1]))


def attend_kernel(
    pieces, new_tokens, w_query, w_key, w_value, w_decay, bias, gain, head_gain, prompt_state, decode_state, w_out,
    acc, peer, w_last, prompt_out, dec_new,
    x3, nt, wq, wk, wv, wd, bias_v, gain_v, hg_v, ps, ds, wo, xs, rows, qb, kb, vb, db, bb, st, tt, ttt, rs, rt, sb, inc,
    att, sqc, nrm, peer0, load_sem, wo_sem, row_sem, st_send, st_recv, tt_send, tt_recv, in_send, in_recv, nrm_sem,
):
    kv = lax.axis_index("kv")
    tp = lax.axis_index("tp")
    other = 1 - tp
    width = rows.shape[-1]

    def load(i, src, dst):
        return pltpu.make_async_copy(src, dst, load_sem.at[i])

    load_x = load(0, pieces, x3)
    load_nt = load(1, new_tokens, nt)
    load_gain = load(2, gain, gain_v)
    load_d = load(3, w_decay, wd)
    load_k = load(4, w_key, wk)
    load_v = load(5, w_value, wv)
    load_bias = load(6, bias, bias_v)
    load_q = load(7, w_query, wq)
    load_ps = load(8, prompt_state, ps)
    load_ds = load(9, decode_state, ds)
    load_hg = load(10, head_gain, hg_v)
    for copy in (load_x, load_nt, load_gain, load_bias, load_d):
        copy.start()

    barrier = pltpu.get_barrier_semaphore()
    pl.semaphore_signal(barrier, inc=1, device_id={"tp": other}, device_id_type=MESH)
    z, y = kv // SIDE, kv % SIDE
    peers = [lax.rem(z + dz, SIDE) * SIDE + lax.rem(y + dy, SIDE) for dz, dy in by_distance()]
    for to in peers:
        pl.semaphore_signal(barrier, inc=1, device_id={"kv": to}, device_id_type=MESH)

    order = order_matrix()
    for copy in (load_x, load_nt, load_gain):
        copy.wait()
    for copy in (load_k, load_v):
        copy.start()
    flat = x3[...].reshape(RP, width)
    step = 512
    squares = jnp.zeros((RP, 1), F32)
    for c in range(width // step):
        part = dot(order, flat[:, c * step : (c + 1) * step])
        xs[:, c * step : (c + 1) * step] = part
        squares += jnp.sum(part * part, axis=-1, keepdims=True)
    factor = lax.rsqrt(squares / width + EPS)
    for c in range(width // step):
        cols = slice(c * step, (c + 1) * step)
        rows[tp, :RP, cols] = (xs[:, cols] * factor * gain_v[:, cols]).astype(BF16)
    wide = nt[...].astype(F32)
    nt_factor = lax.rsqrt(jnp.sum(wide * wide, axis=-1, keepdims=True) / width + EPS)
    nt_rows = wide * nt_factor * gain_v[...]
    rows[tp, RP:, :] = jnp.concatenate([nt_rows, jnp.zeros((PAD - nt_rows.shape[0], width), F32)], axis=0).astype(BF16)

    pl.semaphore_wait(barrier, KVN)
    row_copy = pltpu.make_async_remote_copy(
        src_ref=rows.at[tp], dst_ref=rows.at[tp], send_sem=row_sem.at[0], recv_sem=row_sem.at[1],
        device_id={"tp": other}, device_id_type=MESH,
    )
    row_copy.start()
    for copy in (load_q, load_ds, load_ps, load_hg):
        copy.start()

    def project(half, weights, out, kind, first, count):
        per = 2 * DK

        def tile(j, _):
            cols = pl.ds(pl.multiple_of(j * per, per), per)
            got = dot(rows[half], weights[:, cols])
            if kind == "v":
                out[j, half] = got.astype(BF16)
            else:
                for e in range(2):
                    part = got[:, e * DK : (e + 1) * DK]
                    if kind == "q":
                        part = (part * DK**-0.5).astype(BF16)
                    elif kind == "k":
                        part = part.astype(BF16)
                    else:
                        at = pl.multiple_of(tp * (HEADS * DK) + j * per + e * DK, DK)
                        part = log_decay(part + bias_v[:, pl.ds(at, DK)])
                    out[2 * j + e, half] = part
            return 0

        lax.fori_loop(first, first + count, tile, 0)

    load_bias.wait()
    load_d.wait()
    project(tp, wd, db, "d", 0, 2)
    load_k.wait()
    project(tp, wk, kb, "k", 0, 2)
    load_v.wait()
    project(tp, wv, vb, "v", 0, 4)
    row_copy.wait()
    project(other, wd, db, "d", 0, 2)

    t_at = lax.broadcasted_iota(jnp.int32, (OWN, OWN), 0)
    s_at = lax.broadcasted_iota(jnp.int32, (OWN, OWN), 1)
    lower = jnp.where(t_at >= s_at, 1.0, 0.0).astype(BF16)
    lower2 = jnp.concatenate([lower, lower], axis=1)
    tt[...] = jnp.zeros_like(tt)

    for p in range(PR):
        total = jnp.zeros((1, HEADS * DK), F32)
        for half in range(2):
            g = jnp.concatenate([db[h, half, p * OWN : (p + 1) * OWN] for h in range(HEADS)], axis=1)
            hi = g.astype(BF16)
            lo = (g - hi.astype(F32)).astype(BF16)
            got = dot(lower2, jnp.concatenate([hi, lo], axis=0))
            total = total + got[OWN - 1 :]
            for h in range(HEADS):
                bb[h, half, p] = got[:, h * DK : (h + 1) * DK]
        for h in range(HEADS):
            n = (h // 2) * 4 + p * 2 + h % 2
            tt[n : n + 1, :] = total[:, h * DK : (h + 1) * DK]
    ttt[...] = tt[...].T.reshape(KVN, ROW_K, DK)

    def total_copy(to, slot):
        return pltpu.make_async_remote_copy(
            src_ref=ttt.at[to], dst_ref=rt.at[slot], send_sem=tt_send.at[to], recv_sem=tt_recv.at[slot],
            device_id={"kv": to}, device_id_type=MESH,
        )

    def state_copy(s, to, slot):
        return pltpu.make_async_remote_copy(
            src_ref=st.at[s, to], dst_ref=rs.at[s, slot], send_sem=st_send.at[s, to], recv_sem=st_recv.at[s, slot],
            device_id={"kv": to}, device_id_type=MESH,
        )

    def back_copy(s, to, slot):
        return pltpu.make_async_remote_copy(
            src_ref=sb.at[s, to], dst_ref=inc.at[s, slot], send_sem=in_send.at[s, to], recv_sem=in_recv.at[s, slot],
            device_id={"kv": to}, device_id_type=MESH,
        )

    for to in peers:
        total_copy(to, kv).start()
    rt[kv] = ttt[kv]

    for s in range(2):
        project(other, wk, kb, "k", s, 1)
        project(other, wv, vb, "v", 2 * s, 2)
        for p in range(PR):
            at = slice(p * OWN, (p + 1) * OWN)
            for e in range(2):
                h = 2 * s + e
                b0, b1 = bb[h, 0, p], bb[h, 1, p]
                t0, t1 = b0[OWN - 1 :], b1[OWN - 1 :]
                e0 = kb[h, 0, at].astype(F32) * jnp.exp((t0 - b0) + t1)
                e1 = kb[h, 1, at].astype(F32) * jnp.exp(t1 - b1)
                keys = jnp.concatenate([e0.astype(BF16), e1.astype(BF16)], axis=0)
                vals = jnp.concatenate([vb[h, 0, at], vb[h, 1, at]], axis=0)
                state = dotg(keys, vals, TN)
                st[s, :, p * 2 + e] = state.reshape(KVN, ROW_K, DV).astype(BF16)
        for to in peers:
            state_copy(s, to, kv).start()
        rs[s, kv] = st[s, kv]

    quarter = width // 4

    def out_rows(i):
        owner = tp if i < 2 else other
        return w_out.at[pl.ds(pl.multiple_of((2 * owner + i % 2) * quarter, quarter), quarter)]

    out_loads = [pltpu.make_async_copy(out_rows(i), wo.at[i] if i < 3 else w_last, wo_sem.at[i]) for i in range(4)]
    for copy in out_loads:
        copy.start()
    load_q.wait()
    project(0, wq, qb, "q", 0, 2)
    project(1, wq, qb, "q", 0, 2)

    t_in = lax.broadcasted_iota(jnp.int32, (BLK, BLK), 0)
    s_in = lax.broadcasted_iota(jnp.int32, (BLK, BLK), 1)
    keep = t_in >= s_in

    def inside(i, _):
        p, h = (i // 2) % 2, 2 * (i // 4) + i % 2
        at = pl.ds(pl.multiple_of(p * OWN, OWN), OWN)
        ks = [kb[h, half, at].astype(F32) for half in range(2)]
        qs = [qb[h, half, at].astype(F32) for half in range(2)]
        bs = [bb[h, half, p] for half in range(2)]
        vs = [vb[h, half, at] for half in range(2)]
        m0, t0 = bs[0][BLK - 1 : BLK], bs[0][OWN - 1 :]
        m1 = bs[1][BLK - 1 : BLK]
        first = (ks[0][:BLK] * jnp.exp(m0 - bs[0][:BLK])).astype(BF16)
        state1 = dotg(first, vs[0][:BLK], TN)
        second = ks[0] * jnp.exp(t0 - bs[0])
        state2 = dotg(second.astype(BF16), vs[0], TN)
        third = jnp.concatenate(
            [(ks[0] * jnp.exp((t0 - bs[0]) + m1)).astype(BF16), (ks[1][:BLK] * jnp.exp(m1 - bs[1][:BLK])).astype(BF16)], axis=0
        )
        state3 = dotg(third, jnp.concatenate([vs[0], vs[1][:BLK]], axis=0), TN)
        starts = [None, state1, state2, state3]
        for blk in range(4):
            half, lo = blk // 2, (blk % 2) * BLK
            b = bs[half][lo : lo + BLK]
            q = qs[half][lo : lo + BLK]
            k = ks[half][lo : lo + BLK]
            v = vs[half][lo : lo + BLK]
            ref = [jnp.zeros((1, DK), F32) if lo == 0 else bs[half][lo - 1 : lo]]
            for n in range(1, BLK // SUB):
                ref.append(b[n * SUB - 1 : n * SUB])
            zero = jnp.zeros((SUB, DK), BF16)
            q_rows, k_cols = [], []
            for n in range(BLK // SUB):
                end = (n + 1) * SUB
                near_q = (q[n * SUB : end] * jnp.exp(b[n * SUB : end] - ref[n])).astype(BF16)
                near_k = (k[:end] * jnp.exp(ref[n] - b[:end])).astype(BF16)
                q_rows.append(jnp.concatenate([near_q if m == n else zero for m in range(BLK // SUB)], axis=1))
                k_cols.append(jnp.concatenate([near_k] + [zero] * (BLK // SUB - 1 - n), axis=0))
            scores = dotg(jnp.concatenate(q_rows, axis=0), jnp.concatenate(k_cols, axis=1), NT)
            weights = jnp.where(keep, scores, 0.0).astype(BF16)
            if blk == 0:
                out = dot(weights, v)
            else:
                start_q = (q * jnp.exp(b - ref[0])).astype(BF16)
                out = dot(
                    jnp.concatenate([start_q, weights], axis=1),
                    jnp.concatenate([starts[blk].astype(BF16), v], axis=0),
                )
            att[i, half, lo : lo + BLK] = out
        sqc[i, 0] = (qs[0] * jnp.exp(bs[0])).astype(BF16)
        sqc[i, 1] = (qs[1] * jnp.exp(bs[1] + t0)).astype(BF16)
        return 0

    lax.fori_loop(0, PH, inside, 0)

    for copy in (load_ps, load_ds, load_hg):
        copy.wait()

    def normed(out, h):
        scale = lax.rsqrt(jnp.sum(out * out, axis=-1, keepdims=True) / DV + EPS)
        gain_at = pl.multiple_of(tp * (HEADS * DV) + h * DV, DV)
        return (out * scale * hg_v[:, pl.ds(gain_at, DV)]).astype(BF16)

    each = 2
    row = lax.broadcasted_iota(jnp.int32, (PAD, 1), 0)
    tt[...] = jnp.zeros_like(tt)
    for half in range(2):
        for h in range(HEADS):
            q = qb[h, half, RP:].astype(F32)
            k = kb[h, half, RP:].astype(F32)
            v = vb[h, half, RP:].astype(F32)
            eg = jnp.exp(db[h, half, RP:])
            eq = (q * eg).astype(BF16)
            out = jnp.sum(q * k, axis=-1, keepdims=True) * v
            for r in range(each):
                from_state = dot(eq, ds[each * half + r, h].astype(BF16))
                out = out + jnp.where(row == r, from_state, 0.0)
                n = (each * half + r) * HEADS + h
                tt[n : n + 1, :] = eg[r : r + 1]
            nrm[half, h // 2, RP:, (h % 2) * DV : (h % 2 + 1) * DV] = normed(out, h)
    columns = tt[...].T
    for half in range(2):
        for h in range(HEADS):
            for r in range(each):
                token = each * half + r
                key = jnp.where(row == r, kb[h, half, RP:].astype(F32), 0.0).astype(BF16)
                fresh = dotg(key, vb[h, half, RP:], TN)
                n = token * HEADS + h
                dec_new[token, h] = columns[:, n : n + 1] * ds[token, h] + fresh

    for to in peers:
        total_copy(to, to).wait_recv()
    for s in range(2):
        for frm in peers:
            state_copy(s, frm, frm).wait_recv()

        def scan_step(i, state):
            decay = jnp.exp(rt[i])
            after = []
            for m in range(4):
                sb[s, i, m] = state[m].astype(BF16)
                after.append(decay[:, s * 4 + m : s * 4 + m + 1] * state[m] + rs[s, i, m].astype(F32))
            return tuple(after)

        at = [(m // 2) * HEADS + 2 * s + m % 2 for m in range(4)]
        last = lax.fori_loop(0, KVN, scan_step, tuple(ps[n] for n in at))
        for to in peers:
            back_copy(s, to, kv).start()
        inc[s, kv] = sb[s, kv]
        for n, state in zip(at, last):
            prompt_out[n] = state

    def nrm_copy(s):
        return pltpu.make_async_remote_copy(
            src_ref=nrm.at[other, s], dst_ref=peer0 if s == 0 else peer, send_sem=nrm_sem.at[s], recv_sem=nrm_sem.at[2 + s],
            device_id={"tp": other}, device_id_type=MESH,
        )

    def add_product(lhs, weights, fresh):
        left = jnp.concatenate([dotg(order, lhs[:RP], TN).astype(BF16), lhs[RP:]], axis=0)
        tile = 256

        def body(n, _):
            cols = pl.ds(pl.multiple_of(n * tile, tile), tile)
            got = dot(left, weights[:, cols])
            acc[:, cols] = got if fresh else acc[:, cols] + got
            return 0

        lax.fori_loop(0, width // tile, body, 0)

    for s in range(2):
        for frm in peers:
            back_copy(s, frm, frm).wait_recv()
        for p in range(PR):
            for e in range(2):
                m = p * 2 + e
                incoming = inc[s, :, m].astype(F32).reshape(DK, DV).astype(BF16)
                for half in range(2):
                    out = att[4 * s + m, half] + dot(sqc[4 * s + m, half], incoming)
                    nrm[half, s, p * OWN : (p + 1) * OWN, e * DV : (e + 1) * DV] = normed(out, 2 * s + e)
        nrm_copy(s).start()
        out_loads[s].wait()
        add_product(nrm[tp, s], wo.at[s], s == 0)
        nrm_copy(s).wait()
        if s == 0:
            out_loads[2].wait()
            add_product(peer0[...], wo.at[2], False)
    out_loads[3].wait()
    for to in peers:
        total_copy(to, kv).wait_send()
        for s in range(2):
            state_copy(s, to, kv).wait_send()
            back_copy(s, to, kv).wait_send()


def finish_kernel(acc, peer, w_last, prompt_in, dec_in, mixed, mixed_dec, prompt_out, dec_out, out3, out2, sem, tile_sem):
    width = acc.shape[-1]
    copies = [pltpu.make_async_copy(dec_in, dec_out, sem.at[0]), pltpu.make_async_copy(prompt_in, prompt_out, sem.at[1])]
    for copy in copies:
        copy.start()
    order = order_matrix()
    left = jnp.concatenate([dotg(order, peer[:RP], TN).astype(BF16), peer[RP:]], axis=0)
    tile = 256

    def out_copy(n):
        cols = pl.ds(pl.multiple_of(n * tile, tile), tile)
        return pltpu.make_async_copy(out3.at[:, :, cols], mixed.at[:, :, cols], tile_sem.at[n])

    def body(n, _):
        cols = pl.ds(pl.multiple_of(n * tile, tile), tile)
        got = (acc[:, cols] + dot(left, w_last[:, cols])).astype(BF16)
        out3[:, :, cols] = got[:RP].reshape(OWN, PR, tile)
        out2[:, cols] = got[RP : RP + 2]
        out_copy(n).start()
        return 0

    lax.fori_loop(0, width // tile, body, 0)
    last = pltpu.make_async_copy(out2, mixed_dec, sem.at[2])
    last.start()
    for n in range(width // tile):
        out_copy(n).wait()
    last.wait()
    for copy in copies:
        copy.wait()


def on_device(
    pieces, new_tokens, w_query, w_key, w_value, w_decay, decay_bias, norm_gain, head_gain, w_out, prompt_state, decode_state
):
    width = pieces.shape[-1]
    vmem = pl.BlockSpec(memory_space=pltpu.VMEM)
    dma = pltpu.SemaphoreType.DMA
    hbm = pl.BlockSpec(memory_space=pltpu.HBM)
    acc, peer, w_last, prompt_new, dec_new = pl.pallas_call(
        attend_kernel,
        name="attend",
        out_shape=(
            jax.ShapeDtypeStruct((ROWS, width), F32),
            jax.ShapeDtypeStruct((ROWS, 2 * DV), BF16),
            jax.ShapeDtypeStruct((width // 4, width), BF16),
            jax.ShapeDtypeStruct((PH, ROW_K, DV), F32),
            jax.ShapeDtypeStruct((4, HEADS, DK, DV), F32),
        ),
        in_specs=[hbm] * 12,
        out_specs=(vmem,) * 5,
        scratch_shapes=[
            pltpu.VMEM((OWN, PR, width), BF16),
            pltpu.VMEM((2, width), BF16),
            pltpu.VMEM((width, HEADS * DK), BF16),
            pltpu.VMEM((width, HEADS * DK), BF16),
            pltpu.VMEM((width, HEADS * DV), BF16),
            pltpu.VMEM((width, HEADS * DK), BF16),
            pltpu.VMEM((1, 2 * HEADS * DK), F32),
            pltpu.VMEM((1, width), F32),
            pltpu.VMEM((1, width), F32),
            pltpu.VMEM((PH, ROW_K, DV), F32),
            pltpu.VMEM((4, HEADS, DK, DV), F32),
            pltpu.VMEM((3, width // 4, width), BF16),
            pltpu.VMEM((RP, width), F32),
            pltpu.VMEM((2, ROWS, width), BF16),
            pltpu.VMEM((HEADS, 2, ROWS, DK), BF16),
            pltpu.VMEM((HEADS, 2, ROWS, DK), BF16),
            pltpu.VMEM((HEADS, 2, ROWS, DV), BF16),
            pltpu.VMEM((HEADS, 2, ROWS, DK), F32),
            pltpu.VMEM((HEADS, 2, PR, OWN, DK), F32),
            pltpu.VMEM((2, KVN, 4, ROW_K, DV), BF16),
            pltpu.VMEM((DK, DK), F32),
            pltpu.VMEM((KVN, ROW_K, DK), F32),
            pltpu.VMEM((2, KVN, 4, ROW_K, DV), BF16),
            pltpu.VMEM((KVN, ROW_K, DK), F32),
            pltpu.VMEM((2, KVN, 4, ROW_K, DV), BF16),
            pltpu.VMEM((2, KVN, 4, ROW_K, DV), BF16),
            pltpu.VMEM((PH, 2, OWN, DV), F32),
            pltpu.VMEM((PH, 2, OWN, DK), BF16),
            pltpu.VMEM((2, 2, ROWS, 2 * DV), BF16),
            pltpu.VMEM((ROWS, 2 * DV), BF16),
            dma((11,)),
            dma((4,)),
            dma((2,)),
            dma((2, KVN)),
            dma((2, KVN)),
            dma((KVN,)),
            dma((KVN,)),
            dma((2, KVN)),
            dma((2, KVN)),
            dma((4,)),
        ],
        compiler_params=pltpu.CompilerParams(collective_id=0, has_side_effects=True, vmem_limit_bytes=40 * 1024 * 1024),
    )(
        *(
            pltpu.with_memory_space_constraint(a, pltpu.HBM)
            for a in (
                pieces, new_tokens, w_query, w_key, w_value, w_decay, decay_bias.reshape(1, -1), norm_gain.reshape(1, -1),
                head_gain.reshape(1, -1), prompt_state.reshape(PH, ROW_K, DV), decode_state, w_out,
            )
        )
    )
    mixed, mixed_dec, prompt_out, dec_out = pl.pallas_call(
        finish_kernel,
        name="finish",
        out_shape=(
            jax.ShapeDtypeStruct((OWN, PR, width), BF16),
            jax.ShapeDtypeStruct((2, width), BF16),
            jax.ShapeDtypeStruct((PH, ROW_K, DV), F32),
            jax.ShapeDtypeStruct((4, HEADS, DK, DV), F32),
        ),
        in_specs=[vmem] * 5,
        out_specs=(hbm,) * 4,
        scratch_shapes=[
            pltpu.VMEM((OWN, PR, width), BF16),
            pltpu.VMEM((2, width), BF16),
            dma((3,)),
            dma((width // 256,)),
        ],
        compiler_params=pltpu.CompilerParams(vmem_limit_bytes=24 * 1024 * 1024),
    )(acc, peer, w_last, prompt_new, dec_new)
    return (
        mixed,
        mixed_dec,
        prompt_out.reshape(prompt_state.shape),
        dec_out,
    )


def solution(mesh):
    kv_tp, dp_kv_tp = ("kv", "tp"), ("dp", "kv", "tp")
    return jax.shard_map(
        on_device,
        mesh=mesh,
        in_specs=(
            P(kv_tp, "dp", None),
            P(dp_kv_tp, None),
            P(None, "tp"),
            P(None, "tp"),
            P(None, "tp"),
            P(None, "tp"),
            P(),
            P(),
            P(),
            P(),
            P("dp", "tp", "kv", None),
            P(("dp", "kv"), "tp", None, None),
        ),
        out_specs=(
            P(kv_tp, "dp", None),
            P(dp_kv_tp, None),
            P("dp", "tp", "kv", None),
            P(("dp", "kv"), "tp", None, None),
        ),
        check_vma=False,
    )
```

```python
import functools

import jax
import jax.numpy as jnp
from jax import lax
from jax.experimental import pallas as pl
from jax.experimental.pallas import tpu as pltpu
from jax.sharding import PartitionSpec as P

F32 = jnp.float32
BF16 = jnp.bfloat16
MESH = pl.DeviceIdType.MESH

DK = 128
DV = 256
EPS = 0.1
TAU = 16.0
SUB = 16
BLK = 64
HEADS = 4
PR = 2
OWN = 128
PAD = 16
RP = PR * OWN
ROWS = RP + PAD
KVN = 16
SIDE = 4
ROW_K = DK // KVN
PH = PR * HEADS
TN = (((0,), (0,)), ((), ()))
NT = (((1,), (1,)), ((), ()))


def dot(a, b):
    return jnp.dot(a, b, preferred_element_type=F32)


def dotg(a, b, dims):
    return lax.dot_general(a, b, dims, preferred_element_type=F32)


def log_decay(x):
    return (jnp.minimum(x, 0.0) - jnp.log1p(jnp.exp(-jnp.abs(x)))) / TAU


def order_matrix():
    m = lax.broadcasted_iota(jnp.int32, (RP, RP), 0)
    n = lax.broadcasted_iota(jnp.int32, (RP, RP), 1)
    first = jnp.where(m < OWN, PR * m, PR * (m - OWN) + 1)
    return jnp.where(n == first, 1.0, 0.0).astype(BF16)


def by_distance():
    offsets = [(dz, dy) for dz in range(SIDE) for dy in range(SIDE) if dz or dy]
    return sorted(offsets, key=lambda o: -min(o[0], SIDE - o[0]) - min(o[1], SIDE - o[1]))


def attend_kernel(
    pieces, new_tokens, w_query, w_key, w_value, w_decay, bias, gain, head_gain, prompt_state, decode_state, w_out,
    acc, peer, w_last, prompt_out, dec_new,
    x3, nt, wq, wk, wv, wd, bias_v, gain_v, hg_v, ps, ds, wo, xs, rows, qb, kb, vb, db, bb, st, tt, ttt, rs, rt, sb, inc,
    att, sqc, nrm, load_sem, wo_sem, row_sem, st_send, st_recv, tt_send, tt_recv, in_send, in_recv, nrm_sem,
):
    kv = lax.axis_index("kv")
    tp = lax.axis_index("tp")
    other = 1 - tp
    width = rows.shape[-1]

    def load(i, src, dst):
        return pltpu.make_async_copy(src, dst, load_sem.at[i])

    load_x = load(0, pieces, x3)
    load_nt = load(1, new_tokens, nt)
    load_gain = load(2, gain, gain_v)
    load_d = load(3, w_decay, wd)
    load_k = load(4, w_key, wk)
    load_v = load(5, w_value, wv)
    load_bias = load(6, bias, bias_v)
    load_q = load(7, w_query, wq)
    load_ps = load(8, prompt_state, ps)
    load_ds = load(9, decode_state, ds)
    load_hg = load(10, head_gain, hg_v)
    for copy in (load_x, load_nt, load_gain, load_bias, load_d):
        copy.start()

    barrier = pltpu.get_barrier_semaphore()
    pl.semaphore_signal(barrier, inc=1, device_id={"tp": other}, device_id_type=MESH)
    z, y = kv // SIDE, kv % SIDE
    peers = [lax.rem(z + dz, SIDE) * SIDE + lax.rem(y + dy, SIDE) for dz, dy in by_distance()]
    for to in peers:
        pl.semaphore_signal(barrier, inc=1, device_id={"kv": to}, device_id_type=MESH)

    order = order_matrix()
    for copy in (load_x, load_nt, load_gain):
        copy.wait()
    for copy in (load_k, load_v):
        copy.start()
    flat = x3[...].reshape(RP, width)
    step = 512
    squares = jnp.zeros((RP, 1), F32)
    for c in range(width // step):
        part = dot(order, flat[:, c * step : (c + 1) * step])
        xs[:, c * step : (c + 1) * step] = part
        squares += jnp.sum(part * part, axis=-1, keepdims=True)
    factor = lax.rsqrt(squares / width + EPS)
    for c in range(width // step):
        cols = slice(c * step, (c + 1) * step)
        rows[tp, :RP, cols] = (xs[:, cols] * factor * gain_v[:, cols]).astype(BF16)
    wide = nt[...].astype(F32)
    nt_factor = lax.rsqrt(jnp.sum(wide * wide, axis=-1, keepdims=True) / width + EPS)
    nt_rows = wide * nt_factor * gain_v[...]
    rows[tp, RP:, :] = jnp.concatenate([nt_rows, jnp.zeros((PAD - nt_rows.shape[0], width), F32)], axis=0).astype(BF16)

    pl.semaphore_wait(barrier, KVN)
    row_copy = pltpu.make_async_remote_copy(
        src_ref=rows.at[tp], dst_ref=rows.at[tp], send_sem=row_sem.at[0], recv_sem=row_sem.at[1],
        device_id={"tp": other}, device_id_type=MESH,
    )
    row_copy.start()
    for copy in (load_q, load_ds, load_ps, load_hg):
        copy.start()

    def project(half, weights, out, kind, first, count):
        per = 2 * DK

        def tile(j, _):
            cols = pl.ds(pl.multiple_of(j * per, per), per)
            got = dot(rows[half], weights[:, cols])
            if kind == "v":
                out[j, half] = got.astype(BF16)
            else:
                for e in range(2):
                    part = got[:, e * DK : (e + 1) * DK]
                    if kind == "q":
                        part = (part * DK**-0.5).astype(BF16)
                    elif kind == "k":
                        part = part.astype(BF16)
                    else:
                        at = pl.multiple_of(tp * (HEADS * DK) + j * per + e * DK, DK)
                        part = log_decay(part + bias_v[:, pl.ds(at, DK)])
                    out[2 * j + e, half] = part
            return 0

        lax.fori_loop(first, first + count, tile, 0)

    load_bias.wait()
    load_d.wait()
    project(tp, wd, db, "d", 0, 2)
    load_k.wait()
    project(tp, wk, kb, "k", 0, 2)
    load_v.wait()
    project(tp, wv, vb, "v", 0, 4)
    row_copy.wait()
    project(other, wd, db, "d", 0, 2)

    t_at = lax.broadcasted_iota(jnp.int32, (OWN, OWN), 0)
    s_at = lax.broadcasted_iota(jnp.int32, (OWN, OWN), 1)
    lower = jnp.where(t_at >= s_at, 1.0, 0.0).astype(BF16)
    lower2 = jnp.concatenate([lower, lower], axis=1)
    tt[...] = jnp.zeros_like(tt)

    for p in range(PR):
        total = jnp.zeros((1, HEADS * DK), F32)
        for half in range(2):
            g = jnp.concatenate([db[h, half, p * OWN : (p + 1) * OWN] for h in range(HEADS)], axis=1)
            hi = g.astype(BF16)
            lo = (g - hi.astype(F32)).astype(BF16)
            got = dot(lower2, jnp.concatenate([hi, lo], axis=0))
            total = total + got[OWN - 1 :]
            for h in range(HEADS):
                bb[h, half, p] = got[:, h * DK : (h + 1) * DK]
        for h in range(HEADS):
            n = (h // 2) * 4 + p * 2 + h % 2
            tt[n : n + 1, :] = total[:, h * DK : (h + 1) * DK]
    ttt[...] = tt[...].T.reshape(KVN, ROW_K, DK)

    def total_copy(to, slot):
        return pltpu.make_async_remote_copy(
            src_ref=ttt.at[to], dst_ref=rt.at[slot], send_sem=tt_send.at[to], recv_sem=tt_recv.at[slot],
            device_id={"kv": to}, device_id_type=MESH,
        )

    def state_copy(s, to, slot):
        return pltpu.make_async_remote_copy(
            src_ref=st.at[s, to], dst_ref=rs.at[s, slot], send_sem=st_send.at[s, to], recv_sem=st_recv.at[s, slot],
            device_id={"kv": to}, device_id_type=MESH,
        )

    def back_copy(s, to, slot):
        return pltpu.make_async_remote_copy(
            src_ref=sb.at[s, to], dst_ref=inc.at[s, slot], send_sem=in_send.at[s, to], recv_sem=in_recv.at[s, slot],
            device_id={"kv": to}, device_id_type=MESH,
        )

    for to in peers:
        total_copy(to, kv).start()
    rt[kv] = ttt[kv]

    for s in range(2):
        project(other, wk, kb, "k", s, 1)
        project(other, wv, vb, "v", 2 * s, 2)
        for p in range(PR):
            at = slice(p * OWN, (p + 1) * OWN)
            for e in range(2):
                h = 2 * s + e
                b0, b1 = bb[h, 0, p], bb[h, 1, p]
                t0, t1 = b0[OWN - 1 :], b1[OWN - 1 :]
                e0 = kb[h, 0, at].astype(F32) * jnp.exp((t0 - b0) + t1)
                e1 = kb[h, 1, at].astype(F32) * jnp.exp(t1 - b1)
                keys = jnp.concatenate([e0.astype(BF16), e1.astype(BF16)], axis=0)
                vals = jnp.concatenate([vb[h, 0, at], vb[h, 1, at]], axis=0)
                state = dotg(keys, vals, TN)
                st[s, :, p * 2 + e] = state.reshape(KVN, ROW_K, DV).astype(BF16)
        for to in peers:
            state_copy(s, to, kv).start()
        rs[s, kv] = st[s, kv]

    def out_rows(owner):
        return w_out.at[pl.ds(pl.multiple_of(owner * (width // 2), width // 2), width // 2)]

    out_loads = [
        pltpu.make_async_copy(out_rows(tp), wo, wo_sem.at[0]),
        pltpu.make_async_copy(out_rows(other), w_last, wo_sem.at[1]),
    ]
    for copy in out_loads:
        copy.start()
    load_q.wait()
    project(0, wq, qb, "q", 0, 2)
    project(1, wq, qb, "q", 0, 2)

    t_in = lax.broadcasted_iota(jnp.int32, (BLK, BLK), 0)
    s_in = lax.broadcasted_iota(jnp.int32, (BLK, BLK), 1)
    keep = t_in >= s_in

    def inside(i, _):
        p, h = (i // 2) % 2, 2 * (i // 4) + i % 2
        at = pl.ds(pl.multiple_of(p * OWN, OWN), OWN)
        ks = [kb[h, half, at].astype(F32) for half in range(2)]
        qs = [qb[h, half, at].astype(F32) for half in range(2)]
        bs = [bb[h, half, p] for half in range(2)]
        vs = [vb[h, half, at] for half in range(2)]
        m0, t0 = bs[0][BLK - 1 : BLK], bs[0][OWN - 1 :]
        m1 = bs[1][BLK - 1 : BLK]
        first = (ks[0][:BLK] * jnp.exp(m0 - bs[0][:BLK])).astype(BF16)
        state1 = dotg(first, vs[0][:BLK], TN)
        second = ks[0] * jnp.exp(t0 - bs[0])
        state2 = dotg(second.astype(BF16), vs[0], TN)
        third = jnp.concatenate(
            [(ks[0] * jnp.exp((t0 - bs[0]) + m1)).astype(BF16), (ks[1][:BLK] * jnp.exp(m1 - bs[1][:BLK])).astype(BF16)], axis=0
        )
        state3 = dotg(third, jnp.concatenate([vs[0], vs[1][:BLK]], axis=0), TN)
        starts = [None, state1, state2, state3]
        for blk in range(4):
            half, lo = blk // 2, (blk % 2) * BLK
            b = bs[half][lo : lo + BLK]
            q = qs[half][lo : lo + BLK]
            k = ks[half][lo : lo + BLK]
            v = vs[half][lo : lo + BLK]
            ref = [jnp.zeros((1, DK), F32) if lo == 0 else bs[half][lo - 1 : lo]]
            for n in range(1, BLK // SUB):
                ref.append(b[n * SUB - 1 : n * SUB])
            zero = jnp.zeros((SUB, DK), BF16)
            q_rows, k_cols = [], []
            for n in range(BLK // SUB):
                end = (n + 1) * SUB
                near_q = (q[n * SUB : end] * jnp.exp(b[n * SUB : end] - ref[n])).astype(BF16)
                near_k = (k[:end] * jnp.exp(ref[n] - b[:end])).astype(BF16)
                q_rows.append(jnp.concatenate([near_q if m == n else zero for m in range(BLK // SUB)], axis=1))
                k_cols.append(jnp.concatenate([near_k] + [zero] * (BLK // SUB - 1 - n), axis=0))
            scores = dotg(jnp.concatenate(q_rows, axis=0), jnp.concatenate(k_cols, axis=1), NT)
            weights = jnp.where(keep, scores, 0.0).astype(BF16)
            if blk == 0:
                out = dot(weights, v)
            else:
                start_q = (q * jnp.exp(b - ref[0])).astype(BF16)
                out = dot(
                    jnp.concatenate([start_q, weights], axis=1),
                    jnp.concatenate([starts[blk].astype(BF16), v], axis=0),
                )
            att[i, half, lo : lo + BLK] = out
        sqc[i, 0] = (qs[0] * jnp.exp(bs[0])).astype(BF16)
        sqc[i, 1] = (qs[1] * jnp.exp(bs[1] + t0)).astype(BF16)
        return 0

    lax.fori_loop(0, PH // 2, inside, 0)

    def scan(s):
        for frm in peers:
            if s == 0:
                total_copy(frm, frm).wait_recv()
            state_copy(s, frm, frm).wait_recv()
        at = [(m // 2) * HEADS + 2 * s + m % 2 for m in range(4)]
        state = [ps[n] for n in at]
        for i in range(KVN):
            decay = jnp.exp(rt[i])
            for m in range(4):
                sb[s, i, m] = state[m].astype(BF16)
                n = s * 4 + m
                state[m] = decay[:, n : n + 1] * state[m] + rs[s, i, m].astype(F32)
        for to in peers:
            back_copy(s, to, kv).start()
        inc[s, kv] = sb[s, kv]
        for n, last in zip(at, state):
            prompt_out[n] = last

    load_ps.wait()
    scan(0)
    scan(1)
    lax.fori_loop(PH // 2, PH, inside, 0)

    for copy in (load_ds, load_hg):
        copy.wait()

    def normed(out, h):
        scale = lax.rsqrt(jnp.sum(out * out, axis=-1, keepdims=True) / DV + EPS)
        gain_at = pl.multiple_of(tp * (HEADS * DV) + h * DV, DV)
        return (out * scale * hg_v[:, pl.ds(gain_at, DV)]).astype(BF16)

    each = 2
    row = lax.broadcasted_iota(jnp.int32, (PAD, 1), 0)
    tt[...] = jnp.zeros_like(tt)
    for half in range(2):
        for h in range(HEADS):
            q = qb[h, half, RP:].astype(F32)
            k = kb[h, half, RP:].astype(F32)
            v = vb[h, half, RP:].astype(F32)
            eg = jnp.exp(db[h, half, RP:])
            eq = (q * eg).astype(BF16)
            out = jnp.sum(q * k, axis=-1, keepdims=True) * v
            for r in range(each):
                from_state = dot(eq, ds[each * half + r, h].astype(BF16))
                out = out + jnp.where(row == r, from_state, 0.0)
                n = (each * half + r) * HEADS + h
                tt[n : n + 1, :] = eg[r : r + 1]
            nrm[half, h // 2, RP:, (h % 2) * DV : (h % 2 + 1) * DV] = normed(out, h)
    columns = tt[...].T
    for half in range(2):
        for h in range(HEADS):
            for r in range(each):
                token = each * half + r
                key = jnp.where(row == r, kb[h, half, RP:].astype(F32), 0.0).astype(BF16)
                fresh = dotg(key, vb[h, half, RP:], TN)
                n = token * HEADS + h
                dec_new[token, h] = columns[:, n : n + 1] * ds[token, h] + fresh

    def nrm_copy(s):
        return pltpu.make_async_remote_copy(
            src_ref=nrm.at[other, s], dst_ref=peer.at[s], send_sem=nrm_sem.at[s], recv_sem=nrm_sem.at[2 + s],
            device_id={"tp": other}, device_id_type=MESH,
        )

    for s in range(2):
        for frm in peers:
            back_copy(s, frm, frm).wait_recv()
        for p in range(PR):
            for e in range(2):
                m = p * 2 + e
                incoming = inc[s, :, m].astype(F32).reshape(DK, DV).astype(BF16)
                for half in range(2):
                    out = att[4 * s + m, half] + dot(sqc[4 * s + m, half], incoming)
                    nrm[half, s, p * OWN : (p + 1) * OWN, e * DV : (e + 1) * DV] = normed(out, 2 * s + e)
        nrm_copy(s).start()

    for copy in out_loads:
        copy.wait()
    left = in_position_order(order, nrm, tp)
    tile = 256

    def own_product(n, _):
        cols = pl.ds(pl.multiple_of(n * tile, tile), tile)
        acc[:, cols] = dot(left, wo[:, cols])
        return 0

    lax.fori_loop(0, width // tile, own_product, 0)
    for s in range(2):
        nrm_copy(s).wait()
    for to in peers:
        total_copy(to, kv).wait_send()
        for s in range(2):
            state_copy(s, to, kv).wait_send()
            back_copy(s, to, kv).wait_send()


def in_position_order(order, rows_ref, half):
    cut = [rows_ref[half, s] if half is not None else rows_ref[s] for s in range(2)]
    parts = [jnp.concatenate([dotg(order, part[:RP], TN).astype(BF16), part[RP:]], axis=0) for part in cut]
    return jnp.concatenate(parts, axis=1)


def finish_kernel(acc, peer, w_last, prompt_in, dec_in, mixed, mixed_dec, prompt_out, dec_out, out3, out2, sem, tile_sem):
    width = acc.shape[-1]
    copies = [pltpu.make_async_copy(dec_in, dec_out, sem.at[0]), pltpu.make_async_copy(prompt_in, prompt_out, sem.at[1])]
    for copy in copies:
        copy.start()
    order = order_matrix()
    left = in_position_order(order, peer, None)
    tile = 256

    def out_copy(n):
        cols = pl.ds(pl.multiple_of(n * tile, tile), tile)
        return pltpu.make_async_copy(out3.at[:, :, cols], mixed.at[:, :, cols], tile_sem.at[n])

    def body(n, _):
        cols = pl.ds(pl.multiple_of(n * tile, tile), tile)
        got = (acc[:, cols] + dot(left, w_last[:, cols])).astype(BF16)
        out3[:, :, cols] = got[:RP].reshape(OWN, PR, tile)
        out2[:, cols] = got[RP : RP + 2]
        out_copy(n).start()
        return 0

    lax.fori_loop(0, width // tile, body, 0)
    last = pltpu.make_async_copy(out2, mixed_dec, sem.at[2])
    last.start()
    for n in range(width // tile):
        out_copy(n).wait()
    last.wait()
    for copy in copies:
        copy.wait()


def on_device(
    pieces, new_tokens, w_query, w_key, w_value, w_decay, decay_bias, norm_gain, head_gain, w_out, prompt_state, decode_state
):
    width = pieces.shape[-1]
    vmem = pl.BlockSpec(memory_space=pltpu.VMEM)
    dma = pltpu.SemaphoreType.DMA
    hbm = pl.BlockSpec(memory_space=pltpu.HBM)
    acc, peer, w_last, prompt_new, dec_new = pl.pallas_call(
        attend_kernel,
        name="attend",
        out_shape=(
            jax.ShapeDtypeStruct((ROWS, width), F32),
            jax.ShapeDtypeStruct((2, ROWS, 2 * DV), BF16),
            jax.ShapeDtypeStruct((width // 2, width), BF16),
            jax.ShapeDtypeStruct((PH, ROW_K, DV), F32),
            jax.ShapeDtypeStruct((4, HEADS, DK, DV), F32),
        ),
        in_specs=[hbm] * 12,
        out_specs=(vmem,) * 5,
        scratch_shapes=[
            pltpu.VMEM((OWN, PR, width), BF16),
            pltpu.VMEM((2, width), BF16),
            pltpu.VMEM((width, HEADS * DK), BF16),
            pltpu.VMEM((width, HEADS * DK), BF16),
            pltpu.VMEM((width, HEADS * DV), BF16),
            pltpu.VMEM((width, HEADS * DK), BF16),
            pltpu.VMEM((1, 2 * HEADS * DK), F32),
            pltpu.VMEM((1, width), F32),
            pltpu.VMEM((1, width), F32),
            pltpu.VMEM((PH, ROW_K, DV), F32),
            pltpu.VMEM((4, HEADS, DK, DV), F32),
            pltpu.VMEM((width // 2, width), BF16),
            pltpu.VMEM((RP, width), F32),
            pltpu.VMEM((2, ROWS, width), BF16),
            pltpu.VMEM((HEADS, 2, ROWS, DK), BF16),
            pltpu.VMEM((HEADS, 2, ROWS, DK), BF16),
            pltpu.VMEM((HEADS, 2, ROWS, DV), BF16),
            pltpu.VMEM((HEADS, 2, ROWS, DK), F32),
            pltpu.VMEM((HEADS, 2, PR, OWN, DK), F32),
            pltpu.VMEM((2, KVN, 4, ROW_K, DV), BF16),
            pltpu.VMEM((DK, DK), F32),
            pltpu.VMEM((KVN, ROW_K, DK), F32),
            pltpu.VMEM((2, KVN, 4, ROW_K, DV), BF16),
            pltpu.VMEM((KVN, ROW_K, DK), F32),
            pltpu.VMEM((2, KVN, 4, ROW_K, DV), BF16),
            pltpu.VMEM((2, KVN, 4, ROW_K, DV), BF16),
            pltpu.VMEM((PH, 2, OWN, DV), F32),
            pltpu.VMEM((PH, 2, OWN, DK), BF16),
            pltpu.VMEM((2, 2, ROWS, 2 * DV), BF16),
            dma((11,)),
            dma((2,)),
            dma((2,)),
            dma((2, KVN)),
            dma((2, KVN)),
            dma((KVN,)),
            dma((KVN,)),
            dma((2, KVN)),
            dma((2, KVN)),
            dma((4,)),
        ],
        compiler_params=pltpu.CompilerParams(collective_id=0, has_side_effects=True, vmem_limit_bytes=40 * 1024 * 1024),
    )(
        *(
            pltpu.with_memory_space_constraint(a, pltpu.HBM)
            for a in (
                pieces, new_tokens, w_query, w_key, w_value, w_decay, decay_bias.reshape(1, -1), norm_gain.reshape(1, -1),
                head_gain.reshape(1, -1), prompt_state.reshape(PH, ROW_K, DV), decode_state, w_out,
            )
        )
    )
    mixed, mixed_dec, prompt_out, dec_out = pl.pallas_call(
        finish_kernel,
        name="finish",
        out_shape=(
            jax.ShapeDtypeStruct((OWN, PR, width), BF16),
            jax.ShapeDtypeStruct((2, width), BF16),
            jax.ShapeDtypeStruct((PH, ROW_K, DV), F32),
            jax.ShapeDtypeStruct((4, HEADS, DK, DV), F32),
        ),
        in_specs=[vmem] * 5,
        out_specs=(hbm,) * 4,
        scratch_shapes=[
            pltpu.VMEM((OWN, PR, width), BF16),
            pltpu.VMEM((2, width), BF16),
            dma((3,)),
            dma((width // 256,)),
        ],
        compiler_params=pltpu.CompilerParams(vmem_limit_bytes=24 * 1024 * 1024),
    )(acc, peer, w_last, prompt_new, dec_new)
    return (
        mixed,
        mixed_dec,
        prompt_out.reshape(prompt_state.shape),
        dec_out,
    )


def solution(mesh):
    kv_tp, dp_kv_tp = ("kv", "tp"), ("dp", "kv", "tp")
    return jax.shard_map(
        on_device,
        mesh=mesh,
        in_specs=(
            P(kv_tp, "dp", None),
            P(dp_kv_tp, None),
            P(None, "tp"),
            P(None, "tp"),
            P(None, "tp"),
            P(None, "tp"),
            P(),
            P(),
            P(),
            P(),
            P("dp", "tp", "kv", None),
            P(("dp", "kv"), "tp", None, None),
        ),
        out_specs=(
            P(kv_tp, "dp", None),
            P(dp_kv_tp, None),
            P("dp", "tp", "kv", None),
            P(("dp", "kv"), "tp", None, None),
        ),
        check_vma=False,
    )
```

```python
import functools

import jax
import jax.numpy as jnp
from jax import lax
from jax.experimental import pallas as pl
from jax.experimental.pallas import tpu as pltpu
from jax.sharding import PartitionSpec as P

F32 = jnp.float32
BF16 = jnp.bfloat16
MESH = pl.DeviceIdType.MESH

DK = 128
DV = 256
EPS = 0.1
TAU = 16.0
SUB = 16
BLK = 64
HEADS = 4
PR = 2
OWN = 128
PAD = 16
RP = PR * OWN
ROWS = RP + PAD
KVN = 16
SIDE = 4
ROW_K = DK // KVN
PH = PR * HEADS
TN = (((0,), (0,)), ((), ()))
NT = (((1,), (1,)), ((), ()))


def dot(a, b):
    return jnp.dot(a, b, preferred_element_type=F32)


def dotg(a, b, dims):
    return lax.dot_general(a, b, dims, preferred_element_type=F32)


def log_decay(x):
    return (jnp.minimum(x, 0.0) - jnp.log1p(jnp.exp(-jnp.abs(x)))) / TAU


def order_matrix():
    m = lax.broadcasted_iota(jnp.int32, (RP, RP), 0)
    n = lax.broadcasted_iota(jnp.int32, (RP, RP), 1)
    first = jnp.where(m < OWN, PR * m, PR * (m - OWN) + 1)
    return jnp.where(n == first, 1.0, 0.0).astype(BF16)


def by_distance():
    offsets = [(dz, dy) for dz in range(SIDE) for dy in range(SIDE) if dz or dy]
    return sorted(offsets, key=lambda o: -min(o[0], SIDE - o[0]) - min(o[1], SIDE - o[1]))


def attend_kernel(
    pieces, new_tokens, w_query, w_key, w_value, w_decay, bias, gain, head_gain, prompt_state, decode_state, w_out,
    acc, peer, w_last, prompt_out, dec_new,
    x3, nt, wq, wk, wv, wd, bias_v, gain_v, hg_v, ps, ds, wo, xs, rows, qb, kb, vb, db, bb, st, tt, ttt, rs, rt, sb, inc,
    att, sqc, nrm, peer0, load_sem, wo_sem, row_sem, st_send, st_recv, tt_send, tt_recv, in_send, in_recv, nrm_sem,
):
    kv = lax.axis_index("kv")
    tp = lax.axis_index("tp")
    other = 1 - tp
    width = rows.shape[-1]

    def load(i, src, dst):
        return pltpu.make_async_copy(src, dst, load_sem.at[i])

    load_x = load(0, pieces, x3)
    load_nt = load(1, new_tokens, nt)
    load_gain = load(2, gain, gain_v)
    load_d = load(3, w_decay, wd)
    load_k = load(4, w_key, wk)
    load_v = load(5, w_value, wv)
    load_bias = load(6, bias, bias_v)
    load_q = load(7, w_query, wq)
    load_ps = load(8, prompt_state, ps)
    load_ds = load(9, decode_state, ds)
    load_hg = load(10, head_gain, hg_v)
    for copy in (load_x, load_nt, load_gain, load_bias, load_d):
        copy.start()

    barrier = pltpu.get_barrier_semaphore()
    pl.semaphore_signal(barrier, inc=1, device_id={"tp": other}, device_id_type=MESH)
    z, y = kv // SIDE, kv % SIDE
    peers = [lax.rem(z + dz, SIDE) * SIDE + lax.rem(y + dy, SIDE) for dz, dy in by_distance()]
    for to in peers:
        pl.semaphore_signal(barrier, inc=1, device_id={"kv": to}, device_id_type=MESH)

    order = order_matrix()
    for copy in (load_x, load_nt, load_gain):
        copy.wait()
    for copy in (load_k, load_v, load_q):
        copy.start()
    flat = x3[...].reshape(RP, width)
    step = 512
    squares = jnp.zeros((RP, 1), F32)
    for c in range(width // step):
        part = dot(order, flat[:, c * step : (c + 1) * step])
        xs[:, c * step : (c + 1) * step] = part
        squares += jnp.sum(part * part, axis=-1, keepdims=True)
    factor = lax.rsqrt(squares / width + EPS)
    for c in range(width // step):
        cols = slice(c * step, (c + 1) * step)
        rows[tp, :RP, cols] = (xs[:, cols] * factor * gain_v[:, cols]).astype(BF16)
    wide = nt[...].astype(F32)
    nt_factor = lax.rsqrt(jnp.sum(wide * wide, axis=-1, keepdims=True) / width + EPS)
    nt_rows = wide * nt_factor * gain_v[...]
    rows[tp, RP:, :] = jnp.concatenate([nt_rows, jnp.zeros((PAD - nt_rows.shape[0], width), F32)], axis=0).astype(BF16)

    def project(half, weights, out, kind, first, count):
        per = 2 * DK

        for j in range(first, first + count):
            got = dot(rows[half], weights[:, j * per : (j + 1) * per])
            if kind == "v":
                out[j, half] = got.astype(BF16)
                continue
            for e in range(2):
                part = got[:, e * DK : (e + 1) * DK]
                if kind == "q":
                    part = (part * DK**-0.5).astype(BF16)
                elif kind == "k":
                    part = part.astype(BF16)
                else:
                    at = pl.multiple_of(tp * (HEADS * DK) + j * per + e * DK, DK)
                    part = log_decay(part + bias_v[:, pl.ds(at, DK)])
                out[2 * j + e, half] = part

    load_bias.wait()
    load_d.wait()
    project(tp, wd, db, "d", 0, 2)
    pl.semaphore_wait(barrier, KVN)
    row_copy = pltpu.make_async_remote_copy(
        src_ref=rows.at[tp], dst_ref=rows.at[tp], send_sem=row_sem.at[0], recv_sem=row_sem.at[1],
        device_id={"tp": other}, device_id_type=MESH,
    )
    row_copy.start()
    for copy in (load_ds, load_ps, load_hg):
        copy.start()

    load_k.wait()
    project(tp, wk, kb, "k", 0, 2)
    load_v.wait()
    project(tp, wv, vb, "v", 0, 4)
    load_q.wait()
    project(tp, wq, qb, "q", 0, 2)
    row_copy.wait()
    project(other, wd, db, "d", 0, 2)

    t_at = lax.broadcasted_iota(jnp.int32, (OWN, OWN), 0)
    s_at = lax.broadcasted_iota(jnp.int32, (OWN, OWN), 1)
    lower = jnp.where(t_at >= s_at, 1.0, 0.0).astype(BF16)
    lower2 = jnp.concatenate([lower, lower], axis=1)
    tt[...] = jnp.zeros_like(tt)

    for p in range(PR):
        total = jnp.zeros((1, HEADS * DK), F32)
        for half in range(2):
            g = jnp.concatenate([db[h, half, p * OWN : (p + 1) * OWN] for h in range(HEADS)], axis=1)
            hi = g.astype(BF16)
            lo = (g - hi.astype(F32)).astype(BF16)
            got = dot(lower2, jnp.concatenate([hi, lo], axis=0))
            total = total + got[OWN - 1 :]
            for h in range(HEADS):
                bb[h, half, p] = got[:, h * DK : (h + 1) * DK]
        for h in range(HEADS):
            n = (h // 2) * 4 + p * 2 + h % 2
            tt[n : n + 1, :] = total[:, h * DK : (h + 1) * DK]
    ttt[...] = tt[...].T.reshape(KVN, ROW_K, DK)

    def total_copy(to, slot):
        return pltpu.make_async_remote_copy(
            src_ref=ttt.at[to], dst_ref=rt.at[slot], send_sem=tt_send.at[to], recv_sem=tt_recv.at[slot],
            device_id={"kv": to}, device_id_type=MESH,
        )

    def state_copy(s, to, slot):
        return pltpu.make_async_remote_copy(
            src_ref=st.at[s, to], dst_ref=rs.at[s, slot], send_sem=st_send.at[s, to], recv_sem=st_recv.at[s, slot],
            device_id={"kv": to}, device_id_type=MESH,
        )

    def back_copy(s, to, slot):
        return pltpu.make_async_remote_copy(
            src_ref=sb.at[s, to], dst_ref=inc.at[s, slot], send_sem=in_send.at[s, to], recv_sem=in_recv.at[s, slot],
            device_id={"kv": to}, device_id_type=MESH,
        )

    for to in peers:
        total_copy(to, kv).start()
    rt[kv] = ttt[kv]

    for s in range(2):
        project(other, wk, kb, "k", s, 1)
        project(other, wv, vb, "v", 2 * s, 2)
        for p in range(PR):
            at = slice(p * OWN, (p + 1) * OWN)
            for e in range(2):
                h = 2 * s + e
                b0, b1 = bb[h, 0, p], bb[h, 1, p]
                t0, t1 = b0[OWN - 1 :], b1[OWN - 1 :]
                e0 = kb[h, 0, at].astype(F32) * jnp.exp((t0 - b0) + t1)
                e1 = kb[h, 1, at].astype(F32) * jnp.exp(t1 - b1)
                keys = jnp.concatenate([e0.astype(BF16), e1.astype(BF16)], axis=0)
                vals = jnp.concatenate([vb[h, 0, at], vb[h, 1, at]], axis=0)
                state = dotg(keys, vals, TN)
                st[s, :, p * 2 + e] = state.reshape(KVN, ROW_K, DV).astype(BF16)
        for to in peers:
            state_copy(s, to, kv).start()
        rs[s, kv] = st[s, kv]

    quarter = width // 4

    def out_load(i):
        owner = tp if i < 2 else other
        src = w_out.at[pl.ds(pl.multiple_of((2 * owner + i % 2) * quarter, quarter), quarter)]
        dst = wo.at[i * quarter : (i + 1) * quarter] if i < 3 else w_last
        return pltpu.make_async_copy(src, dst, wo_sem.at[i])

    out_loads = [out_load(i) for i in range(4)]
    for copy in out_loads:
        copy.start()
    project(other, wq, qb, "q", 0, 2)

    t_in = lax.broadcasted_iota(jnp.int32, (BLK, BLK), 0)
    s_in = lax.broadcasted_iota(jnp.int32, (BLK, BLK), 1)
    keep = t_in >= s_in

    def inside(i):
        p, h = (i // 2) % 2, 2 * (i // 4) + i % 2
        at = slice(p * OWN, (p + 1) * OWN)
        ks = [kb[h, half, at].astype(F32) for half in range(2)]
        qs = [qb[h, half, at].astype(F32) for half in range(2)]
        bs = [bb[h, half, p] for half in range(2)]
        vs = [vb[h, half, at] for half in range(2)]
        m0, t0 = bs[0][BLK - 1 : BLK], bs[0][OWN - 1 :]
        m1 = bs[1][BLK - 1 : BLK]
        first = (ks[0][:BLK] * jnp.exp(m0 - bs[0][:BLK])).astype(BF16)
        state1 = dotg(first, vs[0][:BLK], TN)
        second = ks[0] * jnp.exp(t0 - bs[0])
        state2 = dotg(second.astype(BF16), vs[0], TN)
        third = jnp.concatenate(
            [(ks[0] * jnp.exp((t0 - bs[0]) + m1)).astype(BF16), (ks[1][:BLK] * jnp.exp(m1 - bs[1][:BLK])).astype(BF16)], axis=0
        )
        state3 = dotg(third, jnp.concatenate([vs[0], vs[1][:BLK]], axis=0), TN)
        starts = [None, state1, state2, state3]
        for blk in range(4):
            half, lo = blk // 2, (blk % 2) * BLK
            b = bs[half][lo : lo + BLK]
            q = qs[half][lo : lo + BLK]
            k = ks[half][lo : lo + BLK]
            v = vs[half][lo : lo + BLK]
            ref = [jnp.zeros((1, DK), F32) if lo == 0 else bs[half][lo - 1 : lo]]
            for n in range(1, BLK // SUB):
                ref.append(b[n * SUB - 1 : n * SUB])
            zero = jnp.zeros((SUB, DK), BF16)
            q_rows, k_cols = [], []
            for n in range(BLK // SUB):
                end = (n + 1) * SUB
                near_q = (q[n * SUB : end] * jnp.exp(b[n * SUB : end] - ref[n])).astype(BF16)
                near_k = (k[:end] * jnp.exp(ref[n] - b[:end])).astype(BF16)
                q_rows.append(jnp.concatenate([near_q if m == n else zero for m in range(BLK // SUB)], axis=1))
                k_cols.append(jnp.concatenate([near_k] + [zero] * (BLK // SUB - 1 - n), axis=0))
            scores = dotg(jnp.concatenate(q_rows, axis=0), jnp.concatenate(k_cols, axis=1), NT)
            weights = jnp.where(keep, scores, 0.0).astype(BF16)
            if blk == 0:
                out = dot(weights, v)
            else:
                start_q = (q * jnp.exp(b - ref[0])).astype(BF16)
                out = dot(
                    jnp.concatenate([start_q, weights], axis=1),
                    jnp.concatenate([starts[blk].astype(BF16), v], axis=0),
                )
            att[i, half, lo : lo + BLK] = out
        sqc[i, 0] = (qs[0] * jnp.exp(bs[0])).astype(BF16)
        sqc[i, 1] = (qs[1] * jnp.exp(bs[1] + t0)).astype(BF16)

    for i in range(PH // 2):
        inside(i)

    def scan(s):
        for frm in peers:
            if s == 0:
                total_copy(frm, frm).wait_recv()
            state_copy(s, frm, frm).wait_recv()
        at = [(m // 2) * HEADS + 2 * s + m % 2 for m in range(4)]
        state = [ps[n] for n in at]
        for i in range(KVN):
            decay = jnp.exp(rt[i])
            for m in range(4):
                sb[s, i, m] = state[m].astype(BF16)
                n = s * 4 + m
                state[m] = decay[:, n : n + 1] * state[m] + rs[s, i, m].astype(F32)
        for to in peers:
            back_copy(s, to, kv).start()
        inc[s, kv] = sb[s, kv]
        for n, last in zip(at, state):
            prompt_out[n] = last

    load_ps.wait()
    scan(0)
    for i in range(PH // 2, PH):
        inside(i)
    scan(1)

    for copy in (load_ds, load_hg):
        copy.wait()

    def normed(out, h):
        scale = lax.rsqrt(jnp.sum(out * out, axis=-1, keepdims=True) / DV + EPS)
        gain_at = pl.multiple_of(tp * (HEADS * DV) + h * DV, DV)
        return (out * scale * hg_v[:, pl.ds(gain_at, DV)]).astype(BF16)

    each = 2
    row = lax.broadcasted_iota(jnp.int32, (PAD, 1), 0)
    tt[...] = jnp.zeros_like(tt)
    for half in range(2):
        for h in range(HEADS):
            q = qb[h, half, RP:].astype(F32)
            k = kb[h, half, RP:].astype(F32)
            v = vb[h, half, RP:].astype(F32)
            eg = jnp.exp(db[h, half, RP:])
            eq = (q * eg).astype(BF16)
            out = jnp.sum(q * k, axis=-1, keepdims=True) * v
            for r in range(each):
                from_state = dot(eq, ds[each * half + r, h].astype(BF16))
                out = out + jnp.where(row == r, from_state, 0.0)
                n = (each * half + r) * HEADS + h
                tt[n : n + 1, :] = eg[r : r + 1]
            nrm[half, h // 2, RP:, (h % 2) * DV : (h % 2 + 1) * DV] = normed(out, h)
    columns = tt[...].T
    for half in range(2):
        for h in range(HEADS):
            for r in range(each):
                token = each * half + r
                key = jnp.where(row == r, kb[h, half, RP:].astype(F32), 0.0).astype(BF16)
                fresh = dotg(key, vb[h, half, RP:], TN)
                n = token * HEADS + h
                dec_new[token, h] = columns[:, n : n + 1] * ds[token, h] + fresh

    def nrm_copy(s):
        return pltpu.make_async_remote_copy(
            src_ref=nrm.at[other, s], dst_ref=peer0 if s == 0 else peer, send_sem=nrm_sem.at[s], recv_sem=nrm_sem.at[2 + s],
            device_id={"tp": other}, device_id_type=MESH,
        )

    tile = 256
    for s in range(2):
        for frm in peers:
            back_copy(s, frm, frm).wait_recv()
        for p in range(PR):
            for e in range(2):
                m = p * 2 + e
                incoming = inc[s, :, m].astype(F32).reshape(DK, DV).astype(BF16)
                for half in range(2):
                    out = att[4 * s + m, half] + dot(sqc[4 * s + m, half], incoming)
                    nrm[half, s, p * OWN : (p + 1) * OWN, e * DV : (e + 1) * DV] = normed(out, 2 * s + e)
        nrm_copy(s).start()
        left = in_position_order(order, nrm[tp, s])
        out_loads[s].wait()
        if s == 0:
            for n in range(width // tile):
                cols = slice(n * tile, (n + 1) * tile)
                acc[:, cols] = dot(left, wo[:quarter, cols])
        else:
            out_loads[2].wait()
            nrm_copy(0).wait()
            left = jnp.concatenate([left, in_position_order(order, peer0[...])], axis=1)
            for n in range(width // tile):
                cols = slice(n * tile, (n + 1) * tile)
                acc[:, cols] += dot(left, wo[quarter:, cols])
    nrm_copy(1).wait()
    out_loads[3].wait()
    for to in peers:
        total_copy(to, kv).wait_send()
        for s in range(2):
            state_copy(s, to, kv).wait_send()
            back_copy(s, to, kv).wait_send()


def in_position_order(order, part):
    return jnp.concatenate([dotg(order, part[:RP], TN).astype(BF16), part[RP:]], axis=0)


def finish_kernel(acc, peer, w_last, prompt_in, dec_in, mixed, mixed_dec, prompt_out, dec_out, out3, out2, sem, tile_sem):
    width = acc.shape[-1]
    copies = [pltpu.make_async_copy(dec_in, dec_out, sem.at[0]), pltpu.make_async_copy(prompt_in, prompt_out, sem.at[1])]
    for copy in copies:
        copy.start()
    order = order_matrix()
    left = in_position_order(order, peer[...])
    tile = 256

    def out_copy(n):
        cols = slice(n * tile, (n + 1) * tile)
        return pltpu.make_async_copy(out3.at[:, :, cols], mixed.at[:, :, cols], tile_sem.at[n])

    for n in range(width // tile):
        cols = slice(n * tile, (n + 1) * tile)
        got = (acc[:, cols] + dot(left, w_last[:, cols])).astype(BF16)
        out3[:, :, cols] = got[:RP].reshape(OWN, PR, tile)
        out2[:, cols] = got[RP : RP + 2]
        out_copy(n).start()

    last = pltpu.make_async_copy(out2, mixed_dec, sem.at[2])
    last.start()
    for n in range(width // tile):
        out_copy(n).wait()
    last.wait()
    for copy in copies:
        copy.wait()


def on_device(
    pieces, new_tokens, w_query, w_key, w_value, w_decay, decay_bias, norm_gain, head_gain, w_out, prompt_state, decode_state
):
    width = pieces.shape[-1]
    vmem = pl.BlockSpec(memory_space=pltpu.VMEM)
    dma = pltpu.SemaphoreType.DMA
    hbm = pl.BlockSpec(memory_space=pltpu.HBM)
    acc, peer, w_last, prompt_new, dec_new = pl.pallas_call(
        attend_kernel,
        name="attend",
        out_shape=(
            jax.ShapeDtypeStruct((ROWS, width), F32),
            jax.ShapeDtypeStruct((ROWS, 2 * DV), BF16),
            jax.ShapeDtypeStruct((width // 4, width), BF16),
            jax.ShapeDtypeStruct((PH, ROW_K, DV), F32),
            jax.ShapeDtypeStruct((4, HEADS, DK, DV), F32),
        ),
        in_specs=[hbm] * 12,
        out_specs=(vmem,) * 5,
        scratch_shapes=[
            pltpu.VMEM((OWN, PR, width), BF16),
            pltpu.VMEM((2, width), BF16),
            pltpu.VMEM((width, HEADS * DK), BF16),
            pltpu.VMEM((width, HEADS * DK), BF16),
            pltpu.VMEM((width, HEADS * DV), BF16),
            pltpu.VMEM((width, HEADS * DK), BF16),
            pltpu.VMEM((1, 2 * HEADS * DK), F32),
            pltpu.VMEM((1, width), F32),
            pltpu.VMEM((1, width), F32),
            pltpu.VMEM((PH, ROW_K, DV), F32),
            pltpu.VMEM((4, HEADS, DK, DV), F32),
            pltpu.VMEM((3 * width // 4, width), BF16),
            pltpu.VMEM((RP, width), F32),
            pltpu.VMEM((2, ROWS, width), BF16),
            pltpu.VMEM((HEADS, 2, ROWS, DK), BF16),
            pltpu.VMEM((HEADS, 2, ROWS, DK), BF16),
            pltpu.VMEM((HEADS, 2, ROWS, DV), BF16),
            pltpu.VMEM((HEADS, 2, ROWS, DK), F32),
            pltpu.VMEM((HEADS, 2, PR, OWN, DK), F32),
            pltpu.VMEM((2, KVN, 4, ROW_K, DV), BF16),
            pltpu.VMEM((DK, DK), F32),
            pltpu.VMEM((KVN, ROW_K, DK), F32),
            pltpu.VMEM((2, KVN, 4, ROW_K, DV), BF16),
            pltpu.VMEM((KVN, ROW_K, DK), F32),
            pltpu.VMEM((2, KVN, 4, ROW_K, DV), BF16),
            pltpu.VMEM((2, KVN, 4, ROW_K, DV), BF16),
            pltpu.VMEM((PH, 2, OWN, DV), F32),
            pltpu.VMEM((PH, 2, OWN, DK), BF16),
            pltpu.VMEM((2, 2, ROWS, 2 * DV), BF16),
            pltpu.VMEM((ROWS, 2 * DV), BF16),
            dma((11,)),
            dma((4,)),
            dma((2,)),
            dma((2, KVN)),
            dma((2, KVN)),
            dma((KVN,)),
            dma((KVN,)),
            dma((2, KVN)),
            dma((2, KVN)),
            dma((4,)),
        ],
        compiler_params=pltpu.CompilerParams(collective_id=0, has_side_effects=True, vmem_limit_bytes=40 * 1024 * 1024),
    )(
        *(
            pltpu.with_memory_space_constraint(a, pltpu.HBM)
            for a in (
                pieces, new_tokens, w_query, w_key, w_value, w_decay, decay_bias.reshape(1, -1), norm_gain.reshape(1, -1),
                head_gain.reshape(1, -1), prompt_state.reshape(PH, ROW_K, DV), decode_state, w_out,
            )
        )
    )
    mixed, mixed_dec, prompt_out, dec_out = pl.pallas_call(
        finish_kernel,
        name="finish",
        out_shape=(
            jax.ShapeDtypeStruct((OWN, PR, width), BF16),
            jax.ShapeDtypeStruct((2, width), BF16),
            jax.ShapeDtypeStruct((PH, ROW_K, DV), F32),
            jax.ShapeDtypeStruct((4, HEADS, DK, DV), F32),
        ),
        in_specs=[vmem] * 5,
        out_specs=(hbm,) * 4,
        scratch_shapes=[
            pltpu.VMEM((OWN, PR, width), BF16),
            pltpu.VMEM((2, width), BF16),
            dma((3,)),
            dma((width // 256,)),
        ],
        compiler_params=pltpu.CompilerParams(vmem_limit_bytes=24 * 1024 * 1024),
    )(acc, peer, w_last, prompt_new, dec_new)
    return (
        mixed,
        mixed_dec,
        prompt_out.reshape(prompt_state.shape),
        dec_out,
    )


def solution(mesh):
    kv_tp, dp_kv_tp = ("kv", "tp"), ("dp", "kv", "tp")
    return jax.shard_map(
        on_device,
        mesh=mesh,
        in_specs=(
            P(kv_tp, "dp", None),
            P(dp_kv_tp, None),
            P(None, "tp"),
            P(None, "tp"),
            P(None, "tp"),
            P(None, "tp"),
            P(),
            P(),
            P(),
            P(),
            P("dp", "tp", "kv", None),
            P(("dp", "kv"), "tp", None, None),
        ),
        out_specs=(
            P(kv_tp, "dp", None),
            P(dp_kv_tp, None),
            P("dp", "tp", "kv", None),
            P(("dp", "kv"), "tp", None, None),
        ),
        check_vma=False,
    )
```

```python
import functools

import jax
import jax.numpy as jnp
from jax import lax
from jax.experimental import pallas as pl
from jax.experimental.pallas import tpu as pltpu
from jax.sharding import PartitionSpec as P

F32 = jnp.float32
BF16 = jnp.bfloat16
MESH = pl.DeviceIdType.MESH

DK = 128
DV = 256
EPS = 0.1
TAU = 16.0
SUB = 16
BLK = 64
HEADS = 4
PR = 2
OWN = 128
PAD = 16
RP = PR * OWN
ROWS = RP + PAD
KVN = 16
SIDE = 4
ROW_K = DK // KVN
PH = PR * HEADS
STAGES = ((0,), (1, 2), (3,))
TN = (((0,), (0,)), ((), ()))
NT = (((1,), (1,)), ((), ()))


def dot(a, b):
    return jnp.dot(a, b, preferred_element_type=F32)


def dotg(a, b, dims):
    return lax.dot_general(a, b, dims, preferred_element_type=F32)


def log_decay(x):
    return (jnp.minimum(x, 0.0) - jnp.log1p(jnp.exp(-jnp.abs(x)))) / TAU


def order_matrix():
    m = lax.broadcasted_iota(jnp.int32, (RP, RP), 0)
    n = lax.broadcasted_iota(jnp.int32, (RP, RP), 1)
    first = jnp.where(m < OWN, PR * m, PR * (m - OWN) + 1)
    return jnp.where(n == first, 1.0, 0.0).astype(BF16)


def by_distance():
    offsets = [(dz, dy) for dz in range(SIDE) for dy in range(SIDE) if dz or dy]
    return sorted(offsets, key=lambda o: -min(o[0], SIDE - o[0]) - min(o[1], SIDE - o[1]))


def attend_kernel(
    pieces, new_tokens, w_query, w_key, w_value, w_decay, bias, gain, head_gain, prompt_state, decode_state, w_out,
    acc, peer, w_last, prompt_out, dec_new,
    x3, nt, wq, wk, wv, wd, bias_v, gain_v, hg_v, ps, ds, wo, xs, rows, qb, kb, vb, db, bb, tt, ttt, rt,
    st0, st1, st2, rs0, rs1, rs2, sb0, sb1, sb2, inc0, inc1, inc2, peer0, peer1,
    att, sqc, nrm, load_sem, wo_sem, row_sem, st_sem, tt_sem, in_sem, nrm_sem,
):
    kv = lax.axis_index("kv")
    tp = lax.axis_index("tp")
    other = 1 - tp
    width = rows.shape[-1]
    st, rs, sb, inc = (st0, st1, st2), (rs0, rs1, rs2), (sb0, sb1, sb2), (inc0, inc1, inc2)

    def load(i, src, dst):
        return pltpu.make_async_copy(src, dst, load_sem.at[i])

    load_x = load(0, pieces, x3)
    load_nt = load(1, new_tokens, nt)
    load_gain = load(2, gain, gain_v)
    load_d = load(3, w_decay, wd)
    load_k = load(4, w_key, wk)
    load_v = load(5, w_value, wv)
    load_bias = load(6, bias, bias_v)
    load_q = load(7, w_query, wq)
    load_ps = load(8, prompt_state, ps)
    load_ds = load(9, decode_state, ds)
    load_hg = load(10, head_gain, hg_v)
    for copy in (load_x, load_nt, load_gain, load_bias, load_d):
        copy.start()

    barrier = pltpu.get_barrier_semaphore()
    pl.semaphore_signal(barrier, inc=1, device_id={"tp": other}, device_id_type=MESH)
    z, y = kv // SIDE, kv % SIDE
    peers = [lax.rem(z + dz, SIDE) * SIDE + lax.rem(y + dy, SIDE) for dz, dy in by_distance()]
    for to in peers:
        pl.semaphore_signal(barrier, inc=1, device_id={"kv": to}, device_id_type=MESH)

    order = order_matrix()
    for copy in (load_x, load_nt, load_gain):
        copy.wait()
    for copy in (load_k, load_v, load_q):
        copy.start()
    flat = x3[...].reshape(RP, width)
    step = 512
    squares = jnp.zeros((RP, 1), F32)
    for c in range(width // step):
        part = dot(order, flat[:, c * step : (c + 1) * step])
        xs[:, c * step : (c + 1) * step] = part
        squares += jnp.sum(part * part, axis=-1, keepdims=True)
    factor = lax.rsqrt(squares / width + EPS)
    for c in range(width // step):
        cols = slice(c * step, (c + 1) * step)
        rows[tp, :RP, cols] = (xs[:, cols] * factor * gain_v[:, cols]).astype(BF16)
    wide = nt[...].astype(F32)
    nt_factor = lax.rsqrt(jnp.sum(wide * wide, axis=-1, keepdims=True) / width + EPS)
    nt_rows = wide * nt_factor * gain_v[...]
    rows[tp, RP:, :] = jnp.concatenate([nt_rows, jnp.zeros((PAD - nt_rows.shape[0], width), F32)], axis=0).astype(BF16)

    def project(half, weights, out, kind, first, count):
        per = 2 * DK

        for j in range(first, first + count):
            got = dot(rows[half], weights[:, j * per : (j + 1) * per])
            if kind == "v":
                out[j, half] = got.astype(BF16)
                continue
            for e in range(2):
                part = got[:, e * DK : (e + 1) * DK]
                if kind == "q":
                    part = (part * DK**-0.5).astype(BF16)
                elif kind == "k":
                    part = part.astype(BF16)
                else:
                    at = pl.multiple_of(tp * (HEADS * DK) + j * per + e * DK, DK)
                    part = log_decay(part + bias_v[:, pl.ds(at, DK)])
                out[2 * j + e, half] = part

    load_bias.wait()
    load_d.wait()
    project(tp, wd, db, "d", 0, 2)
    pl.semaphore_wait(barrier, KVN)
    row_copy = pltpu.make_async_remote_copy(
        src_ref=rows.at[tp], dst_ref=rows.at[tp], send_sem=row_sem.at[0], recv_sem=row_sem.at[1],
        device_id={"tp": other}, device_id_type=MESH,
    )
    row_copy.start()
    for copy in (load_ds, load_ps, load_hg):
        copy.start()

    load_k.wait()
    project(tp, wk, kb, "k", 0, 2)
    load_v.wait()
    project(tp, wv, vb, "v", 0, 4)
    row_copy.wait()
    project(other, wd, db, "d", 0, 2)

    t_at = lax.broadcasted_iota(jnp.int32, (OWN, OWN), 0)
    s_at = lax.broadcasted_iota(jnp.int32, (OWN, OWN), 1)
    lower = jnp.where(t_at >= s_at, 1.0, 0.0).astype(BF16)
    lower2 = jnp.concatenate([lower, lower], axis=1)
    tt[...] = jnp.zeros_like(tt)

    for p in range(PR):
        total = jnp.zeros((1, HEADS * DK), F32)
        for half in range(2):
            g = jnp.concatenate([db[h, half, p * OWN : (p + 1) * OWN] for h in range(HEADS)], axis=1)
            hi = g.astype(BF16)
            lo = (g - hi.astype(F32)).astype(BF16)
            got = dot(lower2, jnp.concatenate([hi, lo], axis=0))
            total = total + got[OWN - 1 :]
            for h in range(HEADS):
                bb[h, half, p] = got[:, h * DK : (h + 1) * DK]
        for h in range(HEADS):
            n = h * PR + p
            tt[n : n + 1, :] = total[:, h * DK : (h + 1) * DK]
    ttt[...] = tt[...].T.reshape(KVN, ROW_K, DK)

    def total_copy(to, slot):
        return pltpu.make_async_remote_copy(
            src_ref=ttt.at[to], dst_ref=rt.at[slot], send_sem=tt_sem.at[0], recv_sem=tt_sem.at[1],
            device_id={"kv": to}, device_id_type=MESH,
        )

    def state_copy(s, to, slot):
        return pltpu.make_async_remote_copy(
            src_ref=st[s].at[to], dst_ref=rs[s].at[slot], send_sem=st_sem.at[0, s], recv_sem=st_sem.at[1, s],
            device_id={"kv": to}, device_id_type=MESH,
        )

    def back_copy(s, to, slot):
        return pltpu.make_async_remote_copy(
            src_ref=sb[s].at[to], dst_ref=inc[s].at[slot], send_sem=in_sem.at[0, s], recv_sem=in_sem.at[1, s],
            device_id={"kv": to}, device_id_type=MESH,
        )

    def wait_all(ref, sem):
        part = ref.at[: KVN - 1]
        pltpu.make_async_copy(part, part, sem).wait()

    for to in peers:
        total_copy(to, kv).start()
    rt[kv] = ttt[kv]

    for s, heads in enumerate(STAGES):
        for h in heads:
            if h in (0, 2):
                project(other, wk, kb, "k", h // 2, 1)
            project(other, wv, vb, "v", h, 1)
        for e, h in enumerate(heads):
            for p in range(PR):
                at = slice(p * OWN, (p + 1) * OWN)
                b0, b1 = bb[h, 0, p], bb[h, 1, p]
                t0, t1 = b0[OWN - 1 :], b1[OWN - 1 :]
                e0 = kb[h, 0, at].astype(F32) * jnp.exp((t0 - b0) + t1)
                e1 = kb[h, 1, at].astype(F32) * jnp.exp(t1 - b1)
                keys = jnp.concatenate([e0.astype(BF16), e1.astype(BF16)], axis=0)
                vals = jnp.concatenate([vb[h, 0, at], vb[h, 1, at]], axis=0)
                state = dotg(keys, vals, TN)
                st[s][:, e * PR + p] = state.reshape(KVN, ROW_K, DV).astype(BF16)
        for to in peers:
            state_copy(s, to, kv).start()
        rs[s][kv] = st[s][kv]

    quarter = width // 4

    def out_load(i):
        owner, first, count = ((tp, 0, 4), (other, 0, 3), (other, 3, 1))[i]
        src = w_out.at[pl.ds(pl.multiple_of(owner * (2 * quarter) + first * DV, DV), count * DV)]
        dst = w_last if i == 2 else wo.at[pl.ds(4 * DV * i, count * DV)]
        return pltpu.make_async_copy(src, dst, wo_sem.at[i])

    out_loads = [out_load(i) for i in range(3)]
    for copy in out_loads:
        copy.start()
    load_q.wait()
    project(tp, wq, qb, "q", 0, 2)
    project(other, wq, qb, "q", 0, 2)

    t_in = lax.broadcasted_iota(jnp.int32, (BLK, BLK), 0)
    s_in = lax.broadcasted_iota(jnp.int32, (BLK, BLK), 1)
    keep = t_in >= s_in

    def inside(i):
        p, h = i % PR, i // PR
        at = slice(p * OWN, (p + 1) * OWN)
        ks = [kb[h, half, at].astype(F32) for half in range(2)]
        qs = [qb[h, half, at].astype(F32) for half in range(2)]
        bs = [bb[h, half, p] for half in range(2)]
        vs = [vb[h, half, at] for half in range(2)]
        m0, t0 = bs[0][BLK - 1 : BLK], bs[0][OWN - 1 :]
        m1 = bs[1][BLK - 1 : BLK]
        first = (ks[0][:BLK] * jnp.exp(m0 - bs[0][:BLK])).astype(BF16)
        state1 = dotg(first, vs[0][:BLK], TN)
        second = ks[0] * jnp.exp(t0 - bs[0])
        state2 = dotg(second.astype(BF16), vs[0], TN)
        third = jnp.concatenate(
            [(ks[0] * jnp.exp((t0 - bs[0]) + m1)).astype(BF16), (ks[1][:BLK] * jnp.exp(m1 - bs[1][:BLK])).astype(BF16)], axis=0
        )
        state3 = dotg(third, jnp.concatenate([vs[0], vs[1][:BLK]], axis=0), TN)
        starts = [None, state1, state2, state3]
        for blk in range(4):
            half, lo = blk // 2, (blk % 2) * BLK
            b = bs[half][lo : lo + BLK]
            q = qs[half][lo : lo + BLK]
            k = ks[half][lo : lo + BLK]
            v = vs[half][lo : lo + BLK]
            ref = [jnp.zeros((1, DK), F32) if lo == 0 else bs[half][lo - 1 : lo]]
            for n in range(1, BLK // SUB):
                ref.append(b[n * SUB - 1 : n * SUB])
            zero = jnp.zeros((SUB, DK), BF16)
            q_rows, k_cols = [], []
            for n in range(BLK // SUB):
                end = (n + 1) * SUB
                near_q = (q[n * SUB : end] * jnp.exp(b[n * SUB : end] - ref[n])).astype(BF16)
                near_k = (k[:end] * jnp.exp(ref[n] - b[:end])).astype(BF16)
                q_rows.append(jnp.concatenate([near_q if m == n else zero for m in range(BLK // SUB)], axis=1))
                k_cols.append(jnp.concatenate([near_k] + [zero] * (BLK // SUB - 1 - n), axis=0))
            scores = dotg(jnp.concatenate(q_rows, axis=0), jnp.concatenate(k_cols, axis=1), NT)
            weights = jnp.where(keep, scores, 0.0).astype(BF16)
            if blk == 0:
                out = dot(weights, v)
            else:
                start_q = (q * jnp.exp(b - ref[0])).astype(BF16)
                out = dot(
                    jnp.concatenate([start_q, weights], axis=1),
                    jnp.concatenate([starts[blk].astype(BF16), v], axis=0),
                )
            att[i, half, lo : lo + BLK] = out
        sqc[i, 0] = (qs[0] * jnp.exp(bs[0])).astype(BF16)
        sqc[i, 1] = (qs[1] * jnp.exp(bs[1] + t0)).astype(BF16)

    for i in range(PH // 2):
        inside(i)

    def scan(s):
        if s == 0:
            wait_all(rt, tt_sem.at[1])
        wait_all(rs[s], st_sem.at[1, s])
        chains = [(e * PR + p, p * HEADS + h, h * PR + p) for e, h in enumerate(STAGES[s]) for p in range(PR)]
        state = [ps[n] for _, n, _ in chains]
        for i in range(KVN):
            decay = jnp.exp(rt[i])
            for j, (m, _, lane) in enumerate(chains):
                sb[s][i, m] = state[j].astype(BF16)
                state[j] = decay[:, lane : lane + 1] * state[j] + rs[s][i, m].astype(F32)
        for to in peers:
            back_copy(s, to, kv).start()
        inc[s][kv] = sb[s][kv]
        for (_, n, _), last in zip(chains, state):
            prompt_out[n] = last

    load_ps.wait()
    scan(0)
    for i in range(PH // 2, PH):
        inside(i)
    scan(1)
    scan(2)

    for copy in (load_ds, load_hg):
        copy.wait()

    def normed(out, h):
        scale = lax.rsqrt(jnp.sum(out * out, axis=-1, keepdims=True) / DV + EPS)
        gain_at = pl.multiple_of(tp * (HEADS * DV) + h * DV, DV)
        return (out * scale * hg_v[:, pl.ds(gain_at, DV)]).astype(BF16)

    each = 2
    row = lax.broadcasted_iota(jnp.int32, (PAD, 1), 0)
    tt[...] = jnp.zeros_like(tt)
    for half in range(2):
        for h in range(HEADS):
            q = qb[h, half, RP:].astype(F32)
            k = kb[h, half, RP:].astype(F32)
            v = vb[h, half, RP:].astype(F32)
            eg = jnp.exp(db[h, half, RP:])
            eq = (q * eg).astype(BF16)
            out = jnp.sum(q * k, axis=-1, keepdims=True) * v
            for r in range(each):
                from_state = dot(eq, ds[each * half + r, h].astype(BF16))
                out = out + jnp.where(row == r, from_state, 0.0)
                n = (each * half + r) * HEADS + h
                tt[n : n + 1, :] = eg[r : r + 1]
            nrm[half, h, RP:] = normed(out, h)
    columns = tt[...].T
    for half in range(2):
        for h in range(HEADS):
            for r in range(each):
                token = each * half + r
                key = jnp.where(row == r, kb[h, half, RP:].astype(F32), 0.0).astype(BF16)
                fresh = dotg(key, vb[h, half, RP:], TN)
                n = token * HEADS + h
                dec_new[token, h] = columns[:, n : n + 1] * ds[token, h] + fresh

    peers_out = (peer0, peer1, peer)

    def nrm_copy(s):
        heads = STAGES[s]
        return pltpu.make_async_remote_copy(
            src_ref=nrm.at[other, heads[0] : heads[-1] + 1], dst_ref=peers_out[s],
            send_sem=nrm_sem.at[0, s], recv_sem=nrm_sem.at[1, s], device_id={"tp": other}, device_id_type=MESH,
        )

    tile = 256
    for s, heads in enumerate(STAGES):
        wait_all(inc[s], in_sem.at[1, s])
        for e, h in enumerate(heads):
            for p in range(PR):
                incoming = inc[s][:, e * PR + p].astype(F32).reshape(DK, DV).astype(BF16)
                for half in range(2):
                    out = att[h * PR + p, half] + dot(sqc[h * PR + p, half], incoming)
                    nrm[half, h, p * OWN : (p + 1) * OWN] = normed(out, h)
        nrm_copy(s).start()
        if s == 1:
            left = in_position_order(order, [nrm[tp, h] for h in range(3)])
            out_loads[0].wait()
            for n in range(width // tile):
                cols = slice(n * tile, (n + 1) * tile)
                acc[:, cols] = dot(left, wo[: 3 * DV, cols])
    out_loads[1].wait()
    for s in range(2):
        nrm_copy(s).wait()
    left = in_position_order(order, [nrm[tp, 3], peer0[0], peer1[0], peer1[1]])
    for n in range(width // tile):
        cols = slice(n * tile, (n + 1) * tile)
        acc[:, cols] += dot(left, wo[3 * DV :, cols])
    nrm_copy(2).wait()
    out_loads[2].wait()
    wait_all(ttt, tt_sem.at[0])
    for s in range(len(STAGES)):
        wait_all(st[s], st_sem.at[0, s])
        wait_all(sb[s], in_sem.at[0, s])


def in_position_order(order, parts):
    cut = [jnp.concatenate([dotg(order, part[:RP], TN).astype(BF16), part[RP:]], axis=0) for part in parts]
    return jnp.concatenate(cut, axis=1)


def finish_kernel(acc, peer, w_last, prompt_in, dec_in, mixed, mixed_dec, prompt_out, dec_out, out3, out2, sem, tile_sem):
    width = acc.shape[-1]
    copies = [pltpu.make_async_copy(dec_in, dec_out, sem.at[0]), pltpu.make_async_copy(prompt_in, prompt_out, sem.at[1])]
    for copy in copies:
        copy.start()
    order = order_matrix()
    left = in_position_order(order, [peer[0]])
    tile = 256

    def out_copy(n):
        cols = slice(n * tile, (n + 1) * tile)
        return pltpu.make_async_copy(out3.at[:, :, cols], mixed.at[:, :, cols], tile_sem.at[n])

    for n in range(width // tile):
        cols = slice(n * tile, (n + 1) * tile)
        got = (acc[:, cols] + dot(left, w_last[:, cols])).astype(BF16)
        out3[:, :, cols] = got[:RP].reshape(OWN, PR, tile)
        out2[:, cols] = got[RP : RP + 2]
        out_copy(n).start()

    last = pltpu.make_async_copy(out2, mixed_dec, sem.at[2])
    last.start()
    for n in range(width // tile):
        out_copy(n).wait()
    last.wait()
    for copy in copies:
        copy.wait()


def on_device(
    pieces, new_tokens, w_query, w_key, w_value, w_decay, decay_bias, norm_gain, head_gain, w_out, prompt_state, decode_state
):
    width = pieces.shape[-1]
    vmem = pl.BlockSpec(memory_space=pltpu.VMEM)
    dma = pltpu.SemaphoreType.DMA
    hbm = pl.BlockSpec(memory_space=pltpu.HBM)
    acc, peer, w_last, prompt_new, dec_new = pl.pallas_call(
        attend_kernel,
        name="attend",
        out_shape=(
            jax.ShapeDtypeStruct((ROWS, width), F32),
            jax.ShapeDtypeStruct((1, ROWS, DV), BF16),
            jax.ShapeDtypeStruct((DV, width), BF16),
            jax.ShapeDtypeStruct((PH, ROW_K, DV), F32),
            jax.ShapeDtypeStruct((4, HEADS, DK, DV), F32),
        ),
        in_specs=[hbm] * 12,
        out_specs=(vmem,) * 5,
        scratch_shapes=[
            pltpu.VMEM((OWN, PR, width), BF16),
            pltpu.VMEM((2, width), BF16),
            pltpu.VMEM((width, HEADS * DK), BF16),
            pltpu.VMEM((width, HEADS * DK), BF16),
            pltpu.VMEM((width, HEADS * DV), BF16),
            pltpu.VMEM((width, HEADS * DK), BF16),
            pltpu.VMEM((1, 2 * HEADS * DK), F32),
            pltpu.VMEM((1, width), F32),
            pltpu.VMEM((1, width), F32),
            pltpu.VMEM((PH, ROW_K, DV), F32),
            pltpu.VMEM((4, HEADS, DK, DV), F32),
            pltpu.VMEM((7 * DV, width), BF16),
            pltpu.VMEM((RP, width), F32),
            pltpu.VMEM((2, ROWS, width), BF16),
            pltpu.VMEM((HEADS, 2, ROWS, DK), BF16),
            pltpu.VMEM((HEADS, 2, ROWS, DK), BF16),
            pltpu.VMEM((HEADS, 2, ROWS, DV), BF16),
            pltpu.VMEM((HEADS, 2, ROWS, DK), F32),
            pltpu.VMEM((HEADS, 2, PR, OWN, DK), F32),
            pltpu.VMEM((DK, DK), F32),
            pltpu.VMEM((KVN, ROW_K, DK), F32),
            pltpu.VMEM((KVN, ROW_K, DK), F32),
            *(pltpu.VMEM((KVN, PR * len(heads), ROW_K, DV), BF16) for _ in range(4) for heads in STAGES),
            *(pltpu.VMEM((len(heads), ROWS, DV), BF16) for heads in STAGES[:2]),
            pltpu.VMEM((PH, 2, OWN, DV), F32),
            pltpu.VMEM((PH, 2, OWN, DK), BF16),
            pltpu.VMEM((2, HEADS, ROWS, DV), BF16),
            dma((11,)),
            dma((3,)),
            dma((2,)),
            dma((2, len(STAGES))),
            dma((2,)),
            dma((2, len(STAGES))),
            dma((2, len(STAGES))),
        ],
        compiler_params=pltpu.CompilerParams(collective_id=0, has_side_effects=True, vmem_limit_bytes=40 * 1024 * 1024),
    )(
        *(
            pltpu.with_memory_space_constraint(a, pltpu.HBM)
            for a in (
                pieces, new_tokens, w_query, w_key, w_value, w_decay, decay_bias.reshape(1, -1), norm_gain.reshape(1, -1),
                head_gain.reshape(1, -1), prompt_state.reshape(PH, ROW_K, DV), decode_state, w_out,
            )
        )
    )
    mixed, mixed_dec, prompt_out, dec_out = pl.pallas_call(
        finish_kernel,
        name="finish",
        out_shape=(
            jax.ShapeDtypeStruct((OWN, PR, width), BF16),
            jax.ShapeDtypeStruct((2, width), BF16),
            jax.ShapeDtypeStruct((PH, ROW_K, DV), F32),
            jax.ShapeDtypeStruct((4, HEADS, DK, DV), F32),
        ),
        in_specs=[vmem] * 5,
        out_specs=(hbm,) * 4,
        scratch_shapes=[
            pltpu.VMEM((OWN, PR, width), BF16),
            pltpu.VMEM((2, width), BF16),
            dma((3,)),
            dma((width // 256,)),
        ],
        compiler_params=pltpu.CompilerParams(vmem_limit_bytes=24 * 1024 * 1024),
    )(acc, peer, w_last, prompt_new, dec_new)
    return (
        mixed,
        mixed_dec,
        prompt_out.reshape(prompt_state.shape),
        dec_out,
    )


def solution(mesh):
    kv_tp, dp_kv_tp = ("kv", "tp"), ("dp", "kv", "tp")
    return jax.shard_map(
        on_device,
        mesh=mesh,
        in_specs=(
            P(kv_tp, "dp", None),
            P(dp_kv_tp, None),
            P(None, "tp"),
            P(None, "tp"),
            P(None, "tp"),
            P(None, "tp"),
            P(),
            P(),
            P(),
            P(),
            P("dp", "tp", "kv", None),
            P(("dp", "kv"), "tp", None, None),
        ),
        out_specs=(
            P(kv_tp, "dp", None),
            P(dp_kv_tp, None),
            P("dp", "tp", "kv", None),
            P(("dp", "kv"), "tp", None, None),
        ),
        check_vma=False,
    )
```

```python
import functools

import jax
import jax.numpy as jnp
from jax import lax
from jax.experimental import pallas as pl
from jax.experimental.pallas import tpu as pltpu
from jax.sharding import PartitionSpec as P

F32 = jnp.float32
BF16 = jnp.bfloat16
MESH = pl.DeviceIdType.MESH

DK = 128
DV = 256
EPS = 0.1
TAU = 16.0
SUB = 16
BLK = 64
HEADS = 4
PR = 2
OWN = 128
PAD = 16
RP = PR * OWN
ROWS = RP + PAD
KVN = 16
SIDE = 4
ROW_K = DK // KVN
PH = PR * HEADS
STAGES = ((0,), (1, 2), (3,))
TN = (((0,), (0,)), ((), ()))
NT = (((1,), (1,)), ((), ()))


def dot(a, b):
    return jnp.dot(a, b, preferred_element_type=F32)


def dotg(a, b, dims):
    return lax.dot_general(a, b, dims, preferred_element_type=F32)


def log_decay(x):
    return (jnp.minimum(x, 0.0) - jnp.log1p(jnp.exp(-jnp.abs(x)))) / TAU


def order_matrix():
    m = lax.broadcasted_iota(jnp.int32, (RP, RP), 0)
    n = lax.broadcasted_iota(jnp.int32, (RP, RP), 1)
    first = jnp.where(m < OWN, PR * m, PR * (m - OWN) + 1)
    return jnp.where(n == first, 1.0, 0.0).astype(BF16)


def by_distance():
    offsets = [(dz, dy) for dz in range(SIDE) for dy in range(SIDE) if dz or dy]
    return sorted(offsets, key=lambda o: -min(o[0], SIDE - o[0]) - min(o[1], SIDE - o[1]))


def attend_kernel(
    pieces, new_tokens, w_query, w_key, w_value, w_decay, bias, gain, head_gain, prompt_state, decode_state, w_out,
    acc, peer, w_last, prompt_out, dec_new,
    x3, nt, wq, wk, wv, wd, bias_v, gain_v, hg_v, ps, ds, wo, xs, rows, qb, kb, vb, db, bb, tt, ttt, rt,
    st0, st1, st2, rs0, rs1, rs2, sb0, sb1, sb2, inc0, inc1, inc2, peer0, peer1,
    att, sqc, nrm, load_sem, wo_sem, row_sem, st_sem, tt_sem, in_sem, nrm_sem,
):
    kv = lax.axis_index("kv")
    tp = lax.axis_index("tp")
    other = 1 - tp
    width = rows.shape[-1]
    st, rs, sb, inc = (st0, st1, st2), (rs0, rs1, rs2), (sb0, sb1, sb2), (inc0, inc1, inc2)

    def load(i, src, dst):
        return pltpu.make_async_copy(src, dst, load_sem.at[i])

    load_x = load(0, pieces, x3)
    load_nt = load(1, new_tokens, nt)
    load_gain = load(2, gain, gain_v)
    load_d = load(3, w_decay, wd)
    load_k = load(4, w_key, wk)
    load_v = load(5, w_value, wv)
    load_bias = load(6, bias, bias_v)
    load_q = load(7, w_query, wq)
    load_ps = load(8, prompt_state, ps)
    load_ds = load(9, decode_state, ds)
    load_hg = load(10, head_gain, hg_v)
    for copy in (load_x, load_nt, load_gain, load_bias, load_d, load_k):
        copy.start()

    barrier = pltpu.get_barrier_semaphore()
    pl.semaphore_signal(barrier, inc=1, device_id={"tp": other}, device_id_type=MESH)
    z, y = kv // SIDE, kv % SIDE
    peers = [lax.rem(z + dz, SIDE) * SIDE + lax.rem(y + dy, SIDE) for dz, dy in by_distance()]
    for to in peers:
        pl.semaphore_signal(barrier, inc=1, device_id={"kv": to}, device_id_type=MESH)

    order = order_matrix()
    for copy in (load_x, load_nt, load_gain):
        copy.wait()
    for copy in (load_v,):
        copy.start()
    flat = x3[...].reshape(RP, width)
    step = 512
    squares = jnp.zeros((RP, 1), F32)
    for c in range(width // step):
        part = dot(order, flat[:, c * step : (c + 1) * step])
        xs[:, c * step : (c + 1) * step] = part
        squares += jnp.sum(part * part, axis=-1, keepdims=True)
    factor = lax.rsqrt(squares / width + EPS)
    for c in range(width // step):
        cols = slice(c * step, (c + 1) * step)
        rows[tp, :RP, cols] = (xs[:, cols] * factor * gain_v[:, cols]).astype(BF16)
    wide = nt[...].astype(F32)
    nt_factor = lax.rsqrt(jnp.sum(wide * wide, axis=-1, keepdims=True) / width + EPS)
    nt_rows = wide * nt_factor * gain_v[...]
    rows[tp, RP:, :] = jnp.concatenate([nt_rows, jnp.zeros((PAD - nt_rows.shape[0], width), F32)], axis=0).astype(BF16)

    def project(half, weights, out, kind, first, count):
        per = 2 * DK

        for j in range(first, first + count):
            got = dot(rows[half], weights[:, j * per : (j + 1) * per])
            if kind == "v":
                out[j, half] = got.astype(BF16)
                continue
            for e in range(2):
                part = got[:, e * DK : (e + 1) * DK]
                if kind == "q":
                    part = (part * DK**-0.5).astype(BF16)
                elif kind == "k":
                    part = part.astype(BF16)
                else:
                    at = pl.multiple_of(tp * (HEADS * DK) + j * per + e * DK, DK)
                    part = log_decay(part + bias_v[:, pl.ds(at, DK)])
                out[2 * j + e, half] = part

    load_bias.wait()
    load_d.wait()
    project(tp, wd, db, "d", 0, 2)
    pl.semaphore_wait(barrier, KVN)
    row_copy = pltpu.make_async_remote_copy(
        src_ref=rows.at[tp], dst_ref=rows.at[tp], send_sem=row_sem.at[0], recv_sem=row_sem.at[1],
        device_id={"tp": other}, device_id_type=MESH,
    )
    row_copy.start()
    for copy in (load_q, load_ds, load_ps, load_hg):
        copy.start()

    load_k.wait()
    project(tp, wk, kb, "k", 0, 2)
    load_v.wait()
    project(tp, wv, vb, "v", 0, 4)
    row_copy.wait()
    project(other, wd, db, "d", 0, 2)

    t_at = lax.broadcasted_iota(jnp.int32, (OWN, OWN), 0)
    s_at = lax.broadcasted_iota(jnp.int32, (OWN, OWN), 1)
    lower = jnp.where(t_at >= s_at, 1.0, 0.0).astype(BF16)
    lower2 = jnp.concatenate([lower, lower], axis=1)
    tt[...] = jnp.zeros_like(tt)

    for p in range(PR):
        total = jnp.zeros((1, HEADS * DK), F32)
        for half in range(2):
            g = jnp.concatenate([db[h, half, p * OWN : (p + 1) * OWN] for h in range(HEADS)], axis=1)
            hi = g.astype(BF16)
            lo = (g - hi.astype(F32)).astype(BF16)
            got = dot(lower2, jnp.concatenate([hi, lo], axis=0))
            total = total + got[OWN - 1 :]
            for h in range(HEADS):
                bb[h, half, p] = got[:, h * DK : (h + 1) * DK]
        for h in range(HEADS):
            n = h * PR + p
            tt[n : n + 1, :] = total[:, h * DK : (h + 1) * DK]
    ttt[...] = tt[...].T.reshape(KVN, ROW_K, DK)

    def total_copy(to, slot):
        return pltpu.make_async_remote_copy(
            src_ref=ttt.at[to], dst_ref=rt.at[slot], send_sem=tt_sem.at[0], recv_sem=tt_sem.at[1],
            device_id={"kv": to}, device_id_type=MESH,
        )

    def state_copy(s, to, slot):
        return pltpu.make_async_remote_copy(
            src_ref=st[s].at[to], dst_ref=rs[s].at[slot], send_sem=st_sem.at[0, s], recv_sem=st_sem.at[1, s],
            device_id={"kv": to}, device_id_type=MESH,
        )

    def back_copy(s, to, slot):
        return pltpu.make_async_remote_copy(
            src_ref=sb[s].at[to], dst_ref=inc[s].at[slot], send_sem=in_sem.at[0, s], recv_sem=in_sem.at[1, s],
            device_id={"kv": to}, device_id_type=MESH,
        )

    def wait_all(ref, sem):
        part = ref.at[: KVN - 1]
        pltpu.make_async_copy(part, part, sem).wait()

    for to in peers:
        total_copy(to, kv).start()
    rt[kv] = ttt[kv]

    for s, heads in enumerate(STAGES):
        if s == 0:
            project(other, wk, kb, "k", 0, 1)
            project(other, wv, vb, "v", 0, 1)
        elif s == 1:
            project(other, wk, kb, "k", 1, 1)
            project(other, wv, vb, "v", 1, 3)
        for e, h in enumerate(heads):
            for p in range(PR):
                at = slice(p * OWN, (p + 1) * OWN)
                b0, b1 = bb[h, 0, p], bb[h, 1, p]
                t0, t1 = b0[OWN - 1 :], b1[OWN - 1 :]
                e0 = kb[h, 0, at].astype(F32) * jnp.exp((t0 - b0) + t1)
                e1 = kb[h, 1, at].astype(F32) * jnp.exp(t1 - b1)
                keys = jnp.concatenate([e0.astype(BF16), e1.astype(BF16)], axis=0)
                vals = jnp.concatenate([vb[h, 0, at], vb[h, 1, at]], axis=0)
                state = dotg(keys, vals, TN)
                st[s][:, e * PR + p] = state.reshape(KVN, ROW_K, DV).astype(BF16)
        for to in peers:
            state_copy(s, to, kv).start()
        rs[s][kv] = st[s][kv]

    quarter = width // 4

    def out_load(i):
        owner, first, count = ((tp, 0, 1), (other, 0, 1), (tp, 1, 3), (other, 1, 2), (other, 3, 1))[i]
        src = w_out.at[pl.ds(pl.multiple_of(owner * (2 * quarter) + first * DV, DV), count * DV)]
        dst = w_last if i == 4 else wo.at[pl.ds((0, 1, 2, 5)[i] * DV, count * DV)]
        return pltpu.make_async_copy(src, dst, wo_sem.at[i])

    out_loads = [out_load(i) for i in range(5)]
    for copy in out_loads:
        copy.start()
    load_q.wait()
    project(tp, wq, qb, "q", 0, 2)
    project(other, wq, qb, "q", 0, 2)

    t_in = lax.broadcasted_iota(jnp.int32, (BLK, BLK), 0)
    s_in = lax.broadcasted_iota(jnp.int32, (BLK, BLK), 1)
    keep = t_in >= s_in

    def inside(i):
        p, h = i % PR, i // PR
        at = slice(p * OWN, (p + 1) * OWN)
        ks = [kb[h, half, at].astype(F32) for half in range(2)]
        qs = [qb[h, half, at].astype(F32) for half in range(2)]
        bs = [bb[h, half, p] for half in range(2)]
        vs = [vb[h, half, at] for half in range(2)]
        m0, t0 = bs[0][BLK - 1 : BLK], bs[0][OWN - 1 :]
        m1 = bs[1][BLK - 1 : BLK]
        first = (ks[0][:BLK] * jnp.exp(m0 - bs[0][:BLK])).astype(BF16)
        state1 = dotg(first, vs[0][:BLK], TN)
        second = ks[0] * jnp.exp(t0 - bs[0])
        state2 = dotg(second.astype(BF16), vs[0], TN)
        third = jnp.concatenate(
            [(ks[0] * jnp.exp((t0 - bs[0]) + m1)).astype(BF16), (ks[1][:BLK] * jnp.exp(m1 - bs[1][:BLK])).astype(BF16)], axis=0
        )
        state3 = dotg(third, jnp.concatenate([vs[0], vs[1][:BLK]], axis=0), TN)
        starts = [None, state1, state2, state3]
        for blk in range(4):
            half, lo = blk // 2, (blk % 2) * BLK
            b = bs[half][lo : lo + BLK]
            q = qs[half][lo : lo + BLK]
            k = ks[half][lo : lo + BLK]
            v = vs[half][lo : lo + BLK]
            ref = [jnp.zeros((1, DK), F32) if lo == 0 else bs[half][lo - 1 : lo]]
            for n in range(1, BLK // SUB):
                ref.append(b[n * SUB - 1 : n * SUB])
            zero = jnp.zeros((SUB, DK), BF16)
            q_rows, k_cols = [], []
            for n in range(BLK // SUB):
                end = (n + 1) * SUB
                near_q = (q[n * SUB : end] * jnp.exp(b[n * SUB : end] - ref[n])).astype(BF16)
                near_k = (k[:end] * jnp.exp(ref[n] - b[:end])).astype(BF16)
                q_rows.append(jnp.concatenate([near_q if m == n else zero for m in range(BLK // SUB)], axis=1))
                k_cols.append(jnp.concatenate([near_k] + [zero] * (BLK // SUB - 1 - n), axis=0))
            scores = dotg(jnp.concatenate(q_rows, axis=0), jnp.concatenate(k_cols, axis=1), NT)
            weights = jnp.where(keep, scores, 0.0).astype(BF16)
            if blk == 0:
                out = dot(weights, v)
            else:
                start_q = (q * jnp.exp(b - ref[0])).astype(BF16)
                out = dot(
                    jnp.concatenate([start_q, weights], axis=1),
                    jnp.concatenate([starts[blk].astype(BF16), v], axis=0),
                )
            att[i, half, lo : lo + BLK] = out
        sqc[i, 0] = (qs[0] * jnp.exp(bs[0])).astype(BF16)
        sqc[i, 1] = (qs[1] * jnp.exp(bs[1] + t0)).astype(BF16)

    for i in range(PH // 2):
        inside(i)

    def scan(s):
        if s == 0:
            wait_all(rt, tt_sem.at[1])
        wait_all(rs[s], st_sem.at[1, s])
        chains = [(e * PR + p, p * HEADS + h, h * PR + p) for e, h in enumerate(STAGES[s]) for p in range(PR)]
        state = [ps[n] for _, n, _ in chains]
        for i in range(KVN):
            decay = jnp.exp(rt[i])
            for j, (m, _, lane) in enumerate(chains):
                sb[s][i, m] = state[j].astype(BF16)
                state[j] = decay[:, lane : lane + 1] * state[j] + rs[s][i, m].astype(F32)
        for to in peers:
            back_copy(s, to, kv).start()
        inc[s][kv] = sb[s][kv]
        for (_, n, _), last in zip(chains, state):
            prompt_out[n] = last

    load_ps.wait()
    scan(0)
    for i in range(PH // 2, PH):
        inside(i)
    scan(1)
    scan(2)

    for copy in (load_ds, load_hg):
        copy.wait()

    def normed(out, h):
        scale = lax.rsqrt(jnp.sum(out * out, axis=-1, keepdims=True) / DV + EPS)
        gain_at = pl.multiple_of(tp * (HEADS * DV) + h * DV, DV)
        return (out * scale * hg_v[:, pl.ds(gain_at, DV)]).astype(BF16)

    each = 2
    row = lax.broadcasted_iota(jnp.int32, (PAD, 1), 0)
    tt[...] = jnp.zeros_like(tt)
    for half in range(2):
        for h in range(HEADS):
            q = qb[h, half, RP:].astype(F32)
            k = kb[h, half, RP:].astype(F32)
            v = vb[h, half, RP:].astype(F32)
            eg = jnp.exp(db[h, half, RP:])
            eq = (q * eg).astype(BF16)
            out = jnp.sum(q * k, axis=-1, keepdims=True) * v
            for r in range(each):
                from_state = dot(eq, ds[each * half + r, h].astype(BF16))
                out = out + jnp.where(row == r, from_state, 0.0)
                n = (each * half + r) * HEADS + h
                tt[n : n + 1, :] = eg[r : r + 1]
            nrm[half, h, RP:] = normed(out, h)
    columns = tt[...].T
    for half in range(2):
        for h in range(HEADS):
            for r in range(each):
                token = each * half + r
                key = jnp.where(row == r, kb[h, half, RP:].astype(F32), 0.0).astype(BF16)
                fresh = dotg(key, vb[h, half, RP:], TN)
                n = token * HEADS + h
                dec_new[token, h] = columns[:, n : n + 1] * ds[token, h] + fresh

    peers_out = (peer0, peer1, peer)

    def nrm_copy(s):
        heads = STAGES[s]
        return pltpu.make_async_remote_copy(
            src_ref=nrm.at[other, heads[0] : heads[-1] + 1], dst_ref=peers_out[s],
            send_sem=nrm_sem.at[0, s], recv_sem=nrm_sem.at[1, s], device_id={"tp": other}, device_id_type=MESH,
        )

    tile = 256
    for s, heads in enumerate(STAGES):
        wait_all(inc[s], in_sem.at[1, s])
        for e, h in enumerate(heads):
            for p in range(PR):
                incoming = inc[s][:, e * PR + p].astype(F32).reshape(DK, DV).astype(BF16)
                for half in range(2):
                    out = att[h * PR + p, half] + dot(sqc[h * PR + p, half], incoming)
                    nrm[half, h, p * OWN : (p + 1) * OWN] = normed(out, h)
        nrm_copy(s).start()
        if s == 0:
            nrm_copy(0).wait()
            parts, at = [nrm[tp, 0], peer0[0]], 0
        elif s == 1:
            parts, at = [nrm[tp, 1], nrm[tp, 2]], 2
        else:
            nrm_copy(1).wait()
            parts, at = [nrm[tp, 3], peer1[0], peer1[1]], 4
        for i in ((0, 1), (2,), (3,))[s]:
            out_loads[i].wait()
        left = in_position_order(order, parts)
        for n in range(width // tile):
            cols = slice(n * tile, (n + 1) * tile)
            got = dot(left, wo[at * DV : (at + len(parts)) * DV, cols])
            acc[:, cols] = acc[:, cols] + got if s else got
    nrm_copy(2).wait()
    out_loads[4].wait()
    wait_all(ttt, tt_sem.at[0])
    for s in range(len(STAGES)):
        wait_all(st[s], st_sem.at[0, s])
        wait_all(sb[s], in_sem.at[0, s])


def in_position_order(order, parts):
    cut = [jnp.concatenate([dotg(order, part[:RP], TN).astype(BF16), part[RP:]], axis=0) for part in parts]
    return jnp.concatenate(cut, axis=1)


def finish_kernel(acc, peer, w_last, prompt_in, dec_in, mixed, mixed_dec, prompt_out, dec_out, out3, out2, sem, tile_sem):
    width = acc.shape[-1]
    copies = [pltpu.make_async_copy(dec_in, dec_out, sem.at[0]), pltpu.make_async_copy(prompt_in, prompt_out, sem.at[1])]
    for copy in copies:
        copy.start()
    order = order_matrix()
    left = in_position_order(order, [peer[0]])
    tile = 256

    def out_copy(n):
        cols = slice(n * tile, (n + 1) * tile)
        return pltpu.make_async_copy(out3.at[:, :, cols], mixed.at[:, :, cols], tile_sem.at[n])

    for n in range(width // tile):
        cols = slice(n * tile, (n + 1) * tile)
        got = (acc[:, cols] + dot(left, w_last[:, cols])).astype(BF16)
        out3[:, :, cols] = got[:RP].reshape(OWN, PR, tile)
        out2[:, cols] = got[RP : RP + 2]
        out_copy(n).start()

    last = pltpu.make_async_copy(out2, mixed_dec, sem.at[2])
    last.start()
    for n in range(width // tile):
        out_copy(n).wait()
    last.wait()
    for copy in copies:
        copy.wait()


def on_device(
    pieces, new_tokens, w_query, w_key, w_value, w_decay, decay_bias, norm_gain, head_gain, w_out, prompt_state, decode_state
):
    width = pieces.shape[-1]
    vmem = pl.BlockSpec(memory_space=pltpu.VMEM)
    dma = pltpu.SemaphoreType.DMA
    hbm = pl.BlockSpec(memory_space=pltpu.HBM)
    acc, peer, w_last, prompt_new, dec_new = pl.pallas_call(
        attend_kernel,
        name="attend",
        out_shape=(
            jax.ShapeDtypeStruct((ROWS, width), F32),
            jax.ShapeDtypeStruct((1, ROWS, DV), BF16),
            jax.ShapeDtypeStruct((DV, width), BF16),
            jax.ShapeDtypeStruct((PH, ROW_K, DV), F32),
            jax.ShapeDtypeStruct((4, HEADS, DK, DV), F32),
        ),
        in_specs=[hbm] * 12,
        out_specs=(vmem,) * 5,
        scratch_shapes=[
            pltpu.VMEM((OWN, PR, width), BF16),
            pltpu.VMEM((2, width), BF16),
            pltpu.VMEM((width, HEADS * DK), BF16),
            pltpu.VMEM((width, HEADS * DK), BF16),
            pltpu.VMEM((width, HEADS * DV), BF16),
            pltpu.VMEM((width, HEADS * DK), BF16),
            pltpu.VMEM((1, 2 * HEADS * DK), F32),
            pltpu.VMEM((1, width), F32),
            pltpu.VMEM((1, width), F32),
            pltpu.VMEM((PH, ROW_K, DV), F32),
            pltpu.VMEM((4, HEADS, DK, DV), F32),
            pltpu.VMEM((7 * DV, width), BF16),
            pltpu.VMEM((RP, width), F32),
            pltpu.VMEM((2, ROWS, width), BF16),
            pltpu.VMEM((HEADS, 2, ROWS, DK), BF16),
            pltpu.VMEM((HEADS, 2, ROWS, DK), BF16),
            pltpu.VMEM((HEADS, 2, ROWS, DV), BF16),
            pltpu.VMEM((HEADS, 2, ROWS, DK), F32),
            pltpu.VMEM((HEADS, 2, PR, OWN, DK), F32),
            pltpu.VMEM((DK, DK), F32),
            pltpu.VMEM((KVN, ROW_K, DK), F32),
            pltpu.VMEM((KVN, ROW_K, DK), F32),
            *(pltpu.VMEM((KVN, PR * len(heads), ROW_K, DV), BF16) for _ in range(4) for heads in STAGES),
            *(pltpu.VMEM((len(heads), ROWS, DV), BF16) for heads in STAGES[:2]),
            pltpu.VMEM((PH, 2, OWN, DV), F32),
            pltpu.VMEM((PH, 2, OWN, DK), BF16),
            pltpu.VMEM((2, HEADS, ROWS, DV), BF16),
            dma((11,)),
            dma((5,)),
            dma((2,)),
            dma((2, len(STAGES))),
            dma((2,)),
            dma((2, len(STAGES))),
            dma((2, len(STAGES))),
        ],
        compiler_params=pltpu.CompilerParams(collective_id=0, has_side_effects=True, vmem_limit_bytes=40 * 1024 * 1024),
    )(
        *(
            pltpu.with_memory_space_constraint(a, pltpu.HBM)
            for a in (
                pieces, new_tokens, w_query, w_key, w_value, w_decay, decay_bias.reshape(1, -1), norm_gain.reshape(1, -1),
                head_gain.reshape(1, -1), prompt_state.reshape(PH, ROW_K, DV), decode_state, w_out,
            )
        )
    )
    mixed, mixed_dec, prompt_out, dec_out = pl.pallas_call(
        finish_kernel,
        name="finish",
        out_shape=(
            jax.ShapeDtypeStruct((OWN, PR, width), BF16),
            jax.ShapeDtypeStruct((2, width), BF16),
            jax.ShapeDtypeStruct((PH, ROW_K, DV), F32),
            jax.ShapeDtypeStruct((4, HEADS, DK, DV), F32),
        ),
        in_specs=[vmem] * 5,
        out_specs=(hbm,) * 4,
        scratch_shapes=[
            pltpu.VMEM((OWN, PR, width), BF16),
            pltpu.VMEM((2, width), BF16),
            dma((3,)),
            dma((width // 256,)),
        ],
        compiler_params=pltpu.CompilerParams(vmem_limit_bytes=24 * 1024 * 1024),
    )(acc, peer, w_last, prompt_new, dec_new)
    return (
        mixed,
        mixed_dec,
        prompt_out.reshape(prompt_state.shape),
        dec_out,
    )


def solution(mesh):
    kv_tp, dp_kv_tp = ("kv", "tp"), ("dp", "kv", "tp")
    return jax.shard_map(
        on_device,
        mesh=mesh,
        in_specs=(
            P(kv_tp, "dp", None),
            P(dp_kv_tp, None),
            P(None, "tp"),
            P(None, "tp"),
            P(None, "tp"),
            P(None, "tp"),
            P(),
            P(),
            P(),
            P(),
            P("dp", "tp", "kv", None),
            P(("dp", "kv"), "tp", None, None),
        ),
        out_specs=(
            P(kv_tp, "dp", None),
            P(dp_kv_tp, None),
            P("dp", "tp", "kv", None),
            P(("dp", "kv"), "tp", None, None),
        ),
        check_vma=False,
    )
```

```python
import functools

import jax
import jax.numpy as jnp
from jax import lax
from jax.experimental import pallas as pl
from jax.experimental.pallas import tpu as pltpu
from jax.sharding import PartitionSpec as P

F32 = jnp.float32
BF16 = jnp.bfloat16
MESH = pl.DeviceIdType.MESH

DK = 128
DV = 256
EPS = 0.1
TAU = 16.0
SUB = 16
BLK = 64
HEADS = 4
PR = 2
OWN = 128
PAD = 16
RP = PR * OWN
ROWS = RP + PAD
KVN = 16
SIDE = 4
ROW_K = DK // KVN
PH = PR * HEADS
STAGES = ((0,), (1, 2), (3,))
TN = (((0,), (0,)), ((), ()))
NT = (((1,), (1,)), ((), ()))


def dot(a, b):
    return jnp.dot(a, b, preferred_element_type=F32)


def dotg(a, b, dims):
    return lax.dot_general(a, b, dims, preferred_element_type=F32)


def log_decay(x):
    return (jnp.minimum(x, 0.0) - jnp.log1p(jnp.exp(-jnp.abs(x)))) / TAU


def order_matrix():
    m = lax.broadcasted_iota(jnp.int32, (RP, RP), 0)
    n = lax.broadcasted_iota(jnp.int32, (RP, RP), 1)
    first = jnp.where(m < OWN, PR * m, PR * (m - OWN) + 1)
    return jnp.where(n == first, 1.0, 0.0).astype(BF16)


def by_distance():
    offsets = [(dz, dy) for dz in range(SIDE) for dy in range(SIDE) if dz or dy]
    return sorted(offsets, key=lambda o: -min(o[0], SIDE - o[0]) - min(o[1], SIDE - o[1]))


def attend_kernel(
    pieces, new_tokens, w_query, w_key, w_value, w_decay, bias, gain, head_gain, prompt_state, decode_state, w_out,
    acc, peer, w_last, prompt_out, dec_new,
    x3, nt, wq, wk, wv, wd, bias_v, gain_v, hg_v, ps, ds, wo, xs, rows, qb, kb, vb, db, bb, tt, ttt, rt,
    st0, st1, st2, rs0, rs1, rs2, sb0, sb1, sb2, inc0, inc1, inc2, peer0, peer1,
    att, sqc, nrm, load_sem, wo_sem, row_sem, st_sem, tt_sem, in_sem, nrm_sem,
):
    kv = lax.axis_index("kv")
    tp = lax.axis_index("tp")
    other = 1 - tp
    width = rows.shape[-1]
    st, rs, sb, inc = (st0, st1, st2), (rs0, rs1, rs2), (sb0, sb1, sb2), (inc0, inc1, inc2)

    def load(i, src, dst):
        return pltpu.make_async_copy(src, dst, load_sem.at[i])

    load_x = load(0, pieces, x3)
    load_nt = load(1, new_tokens, nt)
    load_gain = load(2, gain, gain_v)
    load_d = load(3, w_decay, wd)
    load_k = load(4, w_key, wk)
    load_v = load(5, w_value, wv)
    load_bias = load(6, bias, bias_v)
    load_q = load(7, w_query, wq)
    load_ps = load(8, prompt_state, ps)
    load_ds = load(9, decode_state, ds)
    load_hg = load(10, head_gain, hg_v)
    for copy in (load_x, load_nt, load_gain, load_bias, load_d, load_k):
        copy.start()

    barrier = pltpu.get_barrier_semaphore()
    pl.semaphore_signal(barrier, inc=1, device_id={"tp": other}, device_id_type=MESH)
    z, y = kv // SIDE, kv % SIDE
    peers = [lax.rem(z + dz, SIDE) * SIDE + lax.rem(y + dy, SIDE) for dz, dy in by_distance()]
    for to in peers:
        pl.semaphore_signal(barrier, inc=1, device_id={"kv": to}, device_id_type=MESH)

    order = order_matrix()
    for copy in (load_x, load_nt, load_gain):
        copy.wait()
    for copy in (load_v,):
        copy.start()
    flat = x3[...].reshape(RP, width)
    step = 512
    squares = jnp.zeros((RP, 1), F32)
    for c in range(width // step):
        part = dot(order, flat[:, c * step : (c + 1) * step])
        xs[:, c * step : (c + 1) * step] = part
        squares += jnp.sum(part * part, axis=-1, keepdims=True)
    factor = lax.rsqrt(squares / width + EPS)
    for c in range(width // step):
        cols = slice(c * step, (c + 1) * step)
        rows[tp, :RP, cols] = (xs[:, cols] * factor * gain_v[:, cols]).astype(BF16)
    wide = nt[...].astype(F32)
    nt_factor = lax.rsqrt(jnp.sum(wide * wide, axis=-1, keepdims=True) / width + EPS)
    nt_rows = wide * nt_factor * gain_v[...]
    rows[tp, RP:, :] = jnp.concatenate([nt_rows, jnp.zeros((PAD - nt_rows.shape[0], width), F32)], axis=0).astype(BF16)

    def project(half, weights, out, kind, first, count):
        per = 2 * DK

        for j in range(first, first + count):
            got = dot(rows[half], weights[:, j * per : (j + 1) * per])
            if kind == "v":
                out[j, half] = got.astype(BF16)
                continue
            for e in range(2):
                part = got[:, e * DK : (e + 1) * DK]
                if kind == "q":
                    part = (part * DK**-0.5).astype(BF16)
                elif kind == "k":
                    part = part.astype(BF16)
                else:
                    at = pl.multiple_of(tp * (HEADS * DK) + j * per + e * DK, DK)
                    part = log_decay(part + bias_v[:, pl.ds(at, DK)])
                out[2 * j + e, half] = part

    load_bias.wait()
    load_d.wait()
    project(tp, wd, db, "d", 0, 2)
    pl.semaphore_wait(barrier, KVN)
    row_copy = pltpu.make_async_remote_copy(
        src_ref=rows.at[tp], dst_ref=rows.at[tp], send_sem=row_sem.at[0], recv_sem=row_sem.at[1],
        device_id={"tp": other}, device_id_type=MESH,
    )
    row_copy.start()
    for copy in (load_q, load_ds, load_ps, load_hg):
        copy.start()

    load_k.wait()
    project(tp, wk, kb, "k", 0, 2)
    load_v.wait()
    project(tp, wv, vb, "v", 0, 4)
    row_copy.wait()
    project(other, wd, db, "d", 0, 2)

    t_at = lax.broadcasted_iota(jnp.int32, (OWN, OWN), 0)
    s_at = lax.broadcasted_iota(jnp.int32, (OWN, OWN), 1)
    lower = jnp.where(t_at >= s_at, 1.0, 0.0).astype(BF16)
    lower2 = jnp.concatenate([lower, lower], axis=1)
    tt[...] = jnp.zeros_like(tt)

    for p in range(PR):
        total = jnp.zeros((1, HEADS * DK), F32)
        for half in range(2):
            g = jnp.concatenate([db[h, half, p * OWN : (p + 1) * OWN] for h in range(HEADS)], axis=1)
            hi = g.astype(BF16)
            lo = (g - hi.astype(F32)).astype(BF16)
            got = dot(lower2, jnp.concatenate([hi, lo], axis=0))
            total = total + got[OWN - 1 :]
            for h in range(HEADS):
                bb[h, half, p] = got[:, h * DK : (h + 1) * DK]
        for h in range(HEADS):
            n = h * PR + p
            tt[n : n + 1, :] = total[:, h * DK : (h + 1) * DK]
    ttt[...] = tt[...].T.reshape(KVN, ROW_K, DK)

    def total_copy(to, slot):
        return pltpu.make_async_remote_copy(
            src_ref=ttt.at[to], dst_ref=rt.at[slot], send_sem=tt_sem.at[0], recv_sem=tt_sem.at[1],
            device_id={"kv": to}, device_id_type=MESH,
        )

    def state_copy(s, to, slot):
        return pltpu.make_async_remote_copy(
            src_ref=st[s].at[to], dst_ref=rs[s].at[slot], send_sem=st_sem.at[0, s], recv_sem=st_sem.at[1, s],
            device_id={"kv": to}, device_id_type=MESH,
        )

    def back_copy(s, to, slot):
        return pltpu.make_async_remote_copy(
            src_ref=sb[s].at[to], dst_ref=inc[s].at[slot], send_sem=in_sem.at[0, s], recv_sem=in_sem.at[1, s],
            device_id={"kv": to}, device_id_type=MESH,
        )

    def wait_all(ref, sem):
        part = ref.at[: KVN - 1]
        pltpu.make_async_copy(part, part, sem).wait()

    for to in peers:
        total_copy(to, kv).start()
    rt[kv] = ttt[kv]

    for s, heads in enumerate(STAGES):
        if s == 0:
            project(other, wk, kb, "k", 0, 1)
            project(other, wv, vb, "v", 0, 1)
        elif s == 1:
            project(other, wk, kb, "k", 1, 1)
            project(other, wv, vb, "v", 1, 3)
        for e, h in enumerate(heads):
            for p in range(PR):
                at = slice(p * OWN, (p + 1) * OWN)
                b0, b1 = bb[h, 0, p], bb[h, 1, p]
                t0, t1 = b0[OWN - 1 :], b1[OWN - 1 :]
                e0 = kb[h, 0, at].astype(F32) * jnp.exp((t0 - b0) + t1)
                e1 = kb[h, 1, at].astype(F32) * jnp.exp(t1 - b1)
                keys = jnp.concatenate([e0.astype(BF16), e1.astype(BF16)], axis=0)
                vals = jnp.concatenate([vb[h, 0, at], vb[h, 1, at]], axis=0)
                state = dotg(keys, vals, TN)
                st[s][:, e * PR + p] = state.reshape(KVN, ROW_K, DV).astype(BF16)
        for to in peers:
            state_copy(s, to, kv).start()
        rs[s][kv] = st[s][kv]

    quarter = width // 4

    def out_load(i):
        owner, first, count = ((tp, 0, 1), (other, 0, 1), (tp, 1, 3), (other, 1, 2), (other, 3, 1))[i]
        src = w_out.at[pl.ds(pl.multiple_of(owner * (2 * quarter) + first * DV, DV), count * DV)]
        dst = w_last if i == 4 else wo.at[pl.ds((0, 1, 2, 5)[i] * DV, count * DV)]
        return pltpu.make_async_copy(src, dst, wo_sem.at[i])

    out_loads = [out_load(i) for i in range(5)]
    for copy in out_loads:
        copy.start()
    load_q.wait()
    project(tp, wq, qb, "q", 0, 2)
    project(other, wq, qb, "q", 0, 2)

    t_in = lax.broadcasted_iota(jnp.int32, (BLK, BLK), 0)
    s_in = lax.broadcasted_iota(jnp.int32, (BLK, BLK), 1)
    keep = t_in >= s_in

    def inside(i):
        p, h = i % PR, i // PR
        at = slice(p * OWN, (p + 1) * OWN)
        ks = [kb[h, half, at].astype(F32) for half in range(2)]
        qs = [qb[h, half, at].astype(F32) for half in range(2)]
        bs = [bb[h, half, p] for half in range(2)]
        vs = [vb[h, half, at] for half in range(2)]
        m0, t0 = bs[0][BLK - 1 : BLK], bs[0][OWN - 1 :]
        m1 = bs[1][BLK - 1 : BLK]
        first = (ks[0][:BLK] * jnp.exp(m0 - bs[0][:BLK])).astype(BF16)
        state1 = dotg(first, vs[0][:BLK], TN)
        second = ks[0] * jnp.exp(t0 - bs[0])
        state2 = dotg(second.astype(BF16), vs[0], TN)
        third = jnp.concatenate(
            [(ks[0] * jnp.exp((t0 - bs[0]) + m1)).astype(BF16), (ks[1][:BLK] * jnp.exp(m1 - bs[1][:BLK])).astype(BF16)], axis=0
        )
        state3 = dotg(third, jnp.concatenate([vs[0], vs[1][:BLK]], axis=0), TN)
        starts = [None, state1, state2, state3]
        for blk in range(4):
            half, lo = blk // 2, (blk % 2) * BLK
            b = bs[half][lo : lo + BLK]
            q = qs[half][lo : lo + BLK]
            k = ks[half][lo : lo + BLK]
            v = vs[half][lo : lo + BLK]
            ref = [jnp.zeros((1, DK), F32) if lo == 0 else bs[half][lo - 1 : lo]]
            for n in range(1, BLK // SUB):
                ref.append(b[n * SUB - 1 : n * SUB])
            zero = jnp.zeros((SUB, DK), BF16)
            q_rows, k_cols = [], []
            for n in range(BLK // SUB):
                end = (n + 1) * SUB
                near_q = (q[n * SUB : end] * jnp.exp(b[n * SUB : end] - ref[n])).astype(BF16)
                near_k = (k[:end] * jnp.exp(ref[n] - b[:end])).astype(BF16)
                q_rows.append(jnp.concatenate([near_q if m == n else zero for m in range(BLK // SUB)], axis=1))
                k_cols.append(jnp.concatenate([near_k] + [zero] * (BLK // SUB - 1 - n), axis=0))
            scores = dotg(jnp.concatenate(q_rows, axis=0), jnp.concatenate(k_cols, axis=1), NT)
            weights = jnp.where(keep, scores, 0.0).astype(BF16)
            if blk == 0:
                out = dot(weights, v)
            else:
                start_q = (q * jnp.exp(b - ref[0])).astype(BF16)
                out = dot(
                    jnp.concatenate([start_q, weights], axis=1),
                    jnp.concatenate([starts[blk].astype(BF16), v], axis=0),
                )
            att[i, half, lo : lo + BLK] = out
        sqc[i, 0] = (qs[0] * jnp.exp(bs[0])).astype(BF16)
        sqc[i, 1] = (qs[1] * jnp.exp(bs[1] + t0)).astype(BF16)

    for i in range(PH // 2):
        inside(i)

    def scan(s):
        if s == 0:
            wait_all(rt, tt_sem.at[1])
        wait_all(rs[s], st_sem.at[1, s])
        chains = [(e * PR + p, p * HEADS + h, h * PR + p) for e, h in enumerate(STAGES[s]) for p in range(PR)]
        state = [ps[n] for _, n, _ in chains]
        for i in range(KVN):
            decay = jnp.exp(rt[i])
            for j, (m, _, lane) in enumerate(chains):
                sb[s][i, m] = state[j].astype(BF16)
                state[j] = decay[:, lane : lane + 1] * state[j] + rs[s][i, m].astype(F32)
        for to in peers:
            back_copy(s, to, kv).start()
        inc[s][kv] = sb[s][kv]
        for (_, n, _), last in zip(chains, state):
            prompt_out[n] = last

    load_ps.wait()
    scan(0)
    for i in range(PH // 2, PH):
        inside(i)
    scan(1)

    for copy in (load_ds, load_hg):
        copy.wait()

    def normed(out, h):
        scale = lax.rsqrt(jnp.sum(out * out, axis=-1, keepdims=True) / DV + EPS)
        gain_at = pl.multiple_of(tp * (HEADS * DV) + h * DV, DV)
        return (out * scale * hg_v[:, pl.ds(gain_at, DV)]).astype(BF16)

    each = 2
    row = lax.broadcasted_iota(jnp.int32, (PAD, 1), 0)
    tt[...] = jnp.zeros_like(tt)
    for half in range(2):
        for h in range(HEADS):
            q = qb[h, half, RP:].astype(F32)
            k = kb[h, half, RP:].astype(F32)
            v = vb[h, half, RP:].astype(F32)
            eg = jnp.exp(db[h, half, RP:])
            eq = (q * eg).astype(BF16)
            out = jnp.sum(q * k, axis=-1, keepdims=True) * v
            for r in range(each):
                from_state = dot(eq, ds[each * half + r, h].astype(BF16))
                out = out + jnp.where(row == r, from_state, 0.0)
                n = (each * half + r) * HEADS + h
                tt[n : n + 1, :] = eg[r : r + 1]
            nrm[half, h, RP:] = normed(out, h)
    columns = tt[...].T
    for half in range(2):
        for h in range(HEADS):
            for r in range(each):
                token = each * half + r
                key = jnp.where(row == r, kb[h, half, RP:].astype(F32), 0.0).astype(BF16)
                fresh = dotg(key, vb[h, half, RP:], TN)
                n = token * HEADS + h
                dec_new[token, h] = columns[:, n : n + 1] * ds[token, h] + fresh

    scan(2)
    peers_out = (peer0, peer1, peer)

    def nrm_copy(s):
        heads = STAGES[s]
        return pltpu.make_async_remote_copy(
            src_ref=nrm.at[other, heads[0] : heads[-1] + 1], dst_ref=peers_out[s],
            send_sem=nrm_sem.at[0, s], recv_sem=nrm_sem.at[1, s], device_id={"tp": other}, device_id_type=MESH,
        )

    tile = 256
    for s, heads in enumerate(STAGES):
        wait_all(inc[s], in_sem.at[1, s])
        for e, h in enumerate(heads):
            for p in range(PR):
                incoming = inc[s][:, e * PR + p].astype(F32).reshape(DK, DV).astype(BF16)
                for half in range(2):
                    out = att[h * PR + p, half] + dot(sqc[h * PR + p, half], incoming)
                    nrm[half, h, p * OWN : (p + 1) * OWN] = normed(out, h)
        nrm_copy(s).start()
        if s == 0:
            nrm_copy(0).wait()
            parts, at = [nrm[tp, 0], peer0[0]], 0
        elif s == 1:
            parts, at = [nrm[tp, 1], nrm[tp, 2]], 2
        else:
            nrm_copy(1).wait()
            parts, at = [nrm[tp, 3], peer1[0], peer1[1]], 4
        for i in ((0, 1), (2,), (3,))[s]:
            out_loads[i].wait()
        left = in_position_order(order, parts)
        for n in range(width // tile):
            cols = slice(n * tile, (n + 1) * tile)
            got = dot(left, wo[at * DV : (at + len(parts)) * DV, cols])
            acc[:, cols] = acc[:, cols] + got if s else got
    nrm_copy(2).wait()
    out_loads[4].wait()
    wait_all(ttt, tt_sem.at[0])
    for s in range(len(STAGES)):
        wait_all(st[s], st_sem.at[0, s])
        wait_all(sb[s], in_sem.at[0, s])


def in_position_order(order, parts):
    cut = [jnp.concatenate([dotg(order, part[:RP], TN).astype(BF16), part[RP:]], axis=0) for part in parts]
    return jnp.concatenate(cut, axis=1)


def finish_kernel(acc, peer, w_last, prompt_in, dec_in, mixed, mixed_dec, prompt_out, dec_out, out3, out2, sem, tile_sem):
    width = acc.shape[-1]
    copies = [pltpu.make_async_copy(dec_in, dec_out, sem.at[0]), pltpu.make_async_copy(prompt_in, prompt_out, sem.at[1])]
    for copy in copies:
        copy.start()
    order = order_matrix()
    left = in_position_order(order, [peer[0]])
    tile = 256

    def out_copy(n):
        cols = slice(n * tile, (n + 1) * tile)
        return pltpu.make_async_copy(out3.at[:, :, cols], mixed.at[:, :, cols], tile_sem.at[n])

    for n in range(width // tile):
        cols = slice(n * tile, (n + 1) * tile)
        got = (acc[:, cols] + dot(left, w_last[:, cols])).astype(BF16)
        out3[:, :, cols] = got[:RP].reshape(OWN, PR, tile)
        out2[:, cols] = got[RP : RP + 2]
        out_copy(n).start()

    last = pltpu.make_async_copy(out2, mixed_dec, sem.at[2])
    last.start()
    for n in range(width // tile):
        out_copy(n).wait()
    last.wait()
    for copy in copies:
        copy.wait()


def on_device(
    pieces, new_tokens, w_query, w_key, w_value, w_decay, decay_bias, norm_gain, head_gain, w_out, prompt_state, decode_state
):
    width = pieces.shape[-1]
    vmem = pl.BlockSpec(memory_space=pltpu.VMEM)
    dma = pltpu.SemaphoreType.DMA
    hbm = pl.BlockSpec(memory_space=pltpu.HBM)
    acc, peer, w_last, prompt_new, dec_new = pl.pallas_call(
        attend_kernel,
        name="attend",
        out_shape=(
            jax.ShapeDtypeStruct((ROWS, width), F32),
            jax.ShapeDtypeStruct((1, ROWS, DV), BF16),
            jax.ShapeDtypeStruct((DV, width), BF16),
            jax.ShapeDtypeStruct((PH, ROW_K, DV), F32),
            jax.ShapeDtypeStruct((4, HEADS, DK, DV), F32),
        ),
        in_specs=[hbm] * 12,
        out_specs=(vmem,) * 5,
        scratch_shapes=[
            pltpu.VMEM((OWN, PR, width), BF16),
            pltpu.VMEM((2, width), BF16),
            pltpu.VMEM((width, HEADS * DK), BF16),
            pltpu.VMEM((width, HEADS * DK), BF16),
            pltpu.VMEM((width, HEADS * DV), BF16),
            pltpu.VMEM((width, HEADS * DK), BF16),
            pltpu.VMEM((1, 2 * HEADS * DK), F32),
            pltpu.VMEM((1, width), F32),
            pltpu.VMEM((1, width), F32),
            pltpu.VMEM((PH, ROW_K, DV), F32),
            pltpu.VMEM((4, HEADS, DK, DV), F32),
            pltpu.VMEM((7 * DV, width), BF16),
            pltpu.VMEM((RP, width), F32),
            pltpu.VMEM((2, ROWS, width), BF16),
            pltpu.VMEM((HEADS, 2, ROWS, DK), BF16),
            pltpu.VMEM((HEADS, 2, ROWS, DK), BF16),
            pltpu.VMEM((HEADS, 2, ROWS, DV), BF16),
            pltpu.VMEM((HEADS, 2, ROWS, DK), F32),
            pltpu.VMEM((HEADS, 2, PR, OWN, DK), F32),
            pltpu.VMEM((DK, DK), F32),
            pltpu.VMEM((KVN, ROW_K, DK), F32),
            pltpu.VMEM((KVN, ROW_K, DK), F32),
            *(pltpu.VMEM((KVN, PR * len(heads), ROW_K, DV), BF16) for _ in range(4) for heads in STAGES),
            *(pltpu.VMEM((len(heads), ROWS, DV), BF16) for heads in STAGES[:2]),
            pltpu.VMEM((PH, 2, OWN, DV), F32),
            pltpu.VMEM((PH, 2, OWN, DK), BF16),
            pltpu.VMEM((2, HEADS, ROWS, DV), BF16),
            dma((11,)),
            dma((5,)),
            dma((2,)),
            dma((2, len(STAGES))),
            dma((2,)),
            dma((2, len(STAGES))),
            dma((2, len(STAGES))),
        ],
        compiler_params=pltpu.CompilerParams(collective_id=0, has_side_effects=True, vmem_limit_bytes=40 * 1024 * 1024),
    )(
        *(
            pltpu.with_memory_space_constraint(a, pltpu.HBM)
            for a in (
                pieces, new_tokens, w_query, w_key, w_value, w_decay, decay_bias.reshape(1, -1), norm_gain.reshape(1, -1),
                head_gain.reshape(1, -1), prompt_state.reshape(PH, ROW_K, DV), decode_state, w_out,
            )
        )
    )
    mixed, mixed_dec, prompt_out, dec_out = pl.pallas_call(
        finish_kernel,
        name="finish",
        out_shape=(
            jax.ShapeDtypeStruct((OWN, PR, width), BF16),
            jax.ShapeDtypeStruct((2, width), BF16),
            jax.ShapeDtypeStruct((PH, ROW_K, DV), F32),
            jax.ShapeDtypeStruct((4, HEADS, DK, DV), F32),
        ),
        in_specs=[vmem] * 5,
        out_specs=(hbm,) * 4,
        scratch_shapes=[
            pltpu.VMEM((OWN, PR, width), BF16),
            pltpu.VMEM((2, width), BF16),
            dma((3,)),
            dma((width // 256,)),
        ],
        compiler_params=pltpu.CompilerParams(vmem_limit_bytes=24 * 1024 * 1024),
    )(acc, peer, w_last, prompt_new, dec_new)
    return (
        mixed,
        mixed_dec,
        prompt_out.reshape(prompt_state.shape),
        dec_out,
    )


def solution(mesh):
    kv_tp, dp_kv_tp = ("kv", "tp"), ("dp", "kv", "tp")
    return jax.shard_map(
        on_device,
        mesh=mesh,
        in_specs=(
            P(kv_tp, "dp", None),
            P(dp_kv_tp, None),
            P(None, "tp"),
            P(None, "tp"),
            P(None, "tp"),
            P(None, "tp"),
            P(),
            P(),
            P(),
            P(),
            P("dp", "tp", "kv", None),
            P(("dp", "kv"), "tp", None, None),
        ),
        out_specs=(
            P(kv_tp, "dp", None),
            P(dp_kv_tp, None),
            P("dp", "tp", "kv", None),
            P(("dp", "kv"), "tp", None, None),
        ),
        check_vma=False,
    )
```
